32 devices in a mesh: kv: 8 (over z, y), tp: 4 (over x, core).
Axes of the slice: x: 2, y: 2, z: 4, core: 2. Of those that a mesh axis runs over, the one named last changes fastest.
Arguments:
- block_in: bfloat16 [64, 4096], P(None, ('kv', 'tp')), may hold values from -30 to 30
- before_gain: bfloat16 [4096], P('kv'), may hold values from 0.099609375 to 1.8984375
- before_gate: bfloat16 [4096, 11264], P('kv', 'tp'), may hold values from -0.09375 to 0.09375
- before_up: bfloat16 [4096, 11264], P('kv', 'tp'), may hold values from -0.09375 to 0.09375
- before_down: bfloat16 [11264, 4096], P('tp', 'kv'), may hold values from -0.0546875 to 0.0546875
- mix_gain: bfloat16 [4096], P('kv'), may hold values from 0.099609375 to 1.8984375
- input_gate: bfloat16 [4096, 8192], P('kv', 'tp'), may hold values from -0.09375 to 0.09375
- input_value: bfloat16 [4096, 8192], P('kv', 'tp'), may hold values from -0.09375 to 0.09375
- input_write: bfloat16 [4096, 2048], P('kv', 'tp'), may hold values from -0.09375 to 0.09375
- input_read: bfloat16 [4096, 2048], P('kv', 'tp'), may hold values from -0.09375 to 0.09375
- input_step: bfloat16 [4096, 128], P('kv', 'tp'), may hold values from -0.09375 to 0.09375
- step_bias: float32 [128], P('tp'), may hold values from -3 to 0
- decay_log: float32 [128], P('tp'), may hold values from -1 to 1.4
- skip_gain: float32 [128], P('tp'), may hold values from 0.5 to 2
- value_taps: bfloat16 [4, 8192], P(None, 'tp'), may hold values from -3 to 3
- write_taps: bfloat16 [4, 2048], P(None, 'tp'), may hold values from -3 to 3
- read_taps: bfloat16 [4, 2048], P(None, 'tp'), may hold values from -3 to 3
- value_window: bfloat16 [64, 3, 8192], P('kv', None, 'tp'), may hold values from -6 to 6
- write_window: bfloat16 [64, 3, 2048], P('kv', None, 'tp'), may hold values from -6 to 6
- read_window: bfloat16 [64, 3, 2048], P('kv', None, 'tp'), may hold values from -6 to 6
- scan_state: float32 [64, 128, 64, 128], P('kv', 'tp'), may hold values from -2 to 2
- group_gain: bfloat16 [8192], P('tp'), may hold values from 0.099609375 to 1.8984375
- mixer_out: bfloat16 [8192, 4096], P('tp', 'kv'), may hold values from -0.0625 to 0.0625
- after_gain: bfloat16 [4096], P('kv'), may hold values from 0.099609375 to 1.8984375
- after_gate: bfloat16 [4096, 11264], P('kv', 'tp'), may hold values from -0.09375 to 0.09375
- after_up: bfloat16 [4096, 11264], P('kv', 'tp'), may hold values from -0.09375 to 0.09375
- after_down: bfloat16 [11264, 4096], P('tp', 'kv'), may hold values from -0.0546875 to 0.0546875
Outputs:
- block_out: bfloat16 [64, 4096], P(None, ('kv', 'tp'))
- state_next: float32 [64, 128, 64, 128], P('kv', 'tp')
- value_next: bfloat16 [64, 3, 8192], P('kv', None, 'tp')
- write_next: bfloat16 [64, 3, 2048], P('kv', None, 'tp')
- read_next: bfloat16 [64, 3, 2048], P('kv', None, 'tp')
The draws below stay inside these ranges and needn't reach their ends.
All inputs are finite; a program needn't handle non-finite values.
Results may differ from the reference program's by a relative error of at most 0.0085.
Values may be sent and summed in bfloat16 or wider, within the bound.
A program may use at most 128 MiB of HBM per device.

```python
import math
import jax
import jax.numpy as jnp
from jax import lax

D = 4096
FF = 11264
INNER = 8192
HEAD_DIM = 64
HEADS = 128
GROUPS = 16
STATE = 128
CONV = 4
BATCH = 64
N_KV = 8
N_TP = 4


def draw_block_in(key, part):
    base_key = jax.random.fold_in(key, 11)
    first_key, second_key = jax.random.split(base_key, 2)
    columns = jnp.arange(D, dtype=jnp.int32)
    column_block = D // (N_KV * N_TP)
    tp_place = (columns // column_block % N_TP).astype(jnp.float32)
    column_scale = jnp.exp(1.6 * columns.astype(jnp.float32) / D + 0.7 * tp_place / max(N_TP - 1, 1))
    row_scale = jnp.exp(jax.random.uniform(second_key, (BATCH, 1), jnp.float32, 0.0, 1.1))
    values = jnp.clip(jax.random.normal(first_key, (BATCH, D), jnp.float32), -4.0, 4.0)
    return (0.25 * values * row_scale * column_scale[None, :]).astype(jnp.bfloat16)


def shard_levels(own_key, extent, shards, low, largest):
    loudness = 1.0
    for position, parts in shards:
        heights = jax.random.uniform(jax.random.fold_in(jax.random.fold_in(own_key, 6), position), (parts,), jnp.float32, low / len(shards), largest / len(shards))
        loudness = loudness * jnp.repeat(jnp.exp(heights), extent[position] // parts).reshape((-1,) + (1,) * (len(extent) - 1 - position))
    return loudness


def centred(stream_key, extent, spread, reach, shards=(), kind=jnp.bfloat16):
    entries = spread * jax.random.normal(stream_key, extent, jnp.float32)
    if shards:
        entries = entries * shard_levels(stream_key, extent, shards, -0.22, 0.18)
    return jnp.clip(entries, -reach, reach).astype(kind)


def setup_inputs(seed: int = 0) -> dict:
    arg_keys = jax.random.split(jax.random.key(seed), 28)
    block_in = draw_block_in(jax.random.fold_in(arg_keys[27], 71), 0)
    before_gain = jnp.clip(1.0 + 0.18 * jax.random.normal(arg_keys[1], (D,), jnp.float32), 0.099609375, 1.8984375).astype(jnp.bfloat16)
    before_gate = centred(arg_keys[2], (D, FF), D ** -0.5, 0.09375, ((0, 8), (1, 4)))
    before_up = centred(arg_keys[3], (D, FF), D ** -0.5, 0.09375, ((0, 8), (1, 4)))
    before_down = centred(arg_keys[4], (FF, D), FF ** -0.5, 0.0546875, ((0, 4), (1, 8)))
    mix_gain = jnp.clip(1.0 + 0.18 * jax.random.normal(arg_keys[5], (D,), jnp.float32), 0.099609375, 1.8984375).astype(jnp.bfloat16)
    input_gate = centred(arg_keys[6], (D, INNER), D ** -0.5, 0.09375, ((0, 8), (1, 4)))
    input_value = centred(arg_keys[7], (D, INNER), D ** -0.5, 0.09375, ((0, 8), (1, 4)))
    input_write = centred(arg_keys[8], (D, GROUPS * STATE), D ** -0.5, 0.09375, ((0, 8), (1, 4)))
    input_read = centred(arg_keys[9], (D, GROUPS * STATE), D ** -0.5, 0.09375, ((0, 8), (1, 4)))
    input_step = centred(arg_keys[10], (D, HEADS), D ** -0.5, 0.09375, ((0, 8), (1, 4)))
    step_bias = jnp.clip(-3.0 + 3.0 * jax.random.uniform(arg_keys[11], (HEADS,), jnp.float32) ** shard_levels(arg_keys[11], (HEADS,), ((0, 4),), -0.2, 0.2), -3.0, 0.0)
    decay_log = jnp.clip(-1.0 + 2.4 * jax.random.uniform(arg_keys[12], (HEADS,), jnp.float32) ** shard_levels(arg_keys[12], (HEADS,), ((0, 4),), -0.2, 0.2), -1.0, 1.4)
    skip_gain = jnp.clip(jnp.exp(math.log(2.0) - 1.3862944 * jax.random.uniform(arg_keys[13], (HEADS,), jnp.float32) ** shard_levels(arg_keys[13], (HEADS,), ((0, 4),), -0.2, 0.2)), 0.5, 2.0)
    value_taps = centred(arg_keys[14], (CONV, INNER), CONV ** -0.5, 3.0, ((1, 4),))
    write_taps = centred(arg_keys[15], (CONV, GROUPS * STATE), CONV ** -0.5, 3.0, ((1, 4),))
    read_taps = centred(arg_keys[16], (CONV, GROUPS * STATE), CONV ** -0.5, 3.0, ((1, 4),))
    value_window = centred(arg_keys[17], (BATCH, CONV - 1, INNER), 1.0, 6.0, ((0, 8), (2, 4)))
    write_window = centred(arg_keys[18], (BATCH, CONV - 1, GROUPS * STATE), 1.0, 6.0, ((0, 8), (2, 4)))
    read_window = centred(arg_keys[19], (BATCH, CONV - 1, GROUPS * STATE), 1.0, 6.0, ((0, 8), (2, 4)))
    scan_state = centred(arg_keys[20], (BATCH, HEADS, HEAD_DIM, STATE), 0.3, 2.0, ((0, 8), (1, 4)), jnp.float32)
    group_gain = jnp.clip(1.0 + 0.18 * jax.random.normal(arg_keys[21], (INNER,), jnp.float32), 0.099609375, 1.8984375).astype(jnp.bfloat16)
    mixer_out = centred(arg_keys[22], (INNER, D), INNER ** -0.5, 0.0625, ((0, 4), (1, 8)))
    after_gain = jnp.clip(1.0 + 0.18 * jax.random.normal(arg_keys[23], (D,), jnp.float32), 0.099609375, 1.8984375).astype(jnp.bfloat16)
    after_gate = centred(arg_keys[24], (D, FF), D ** -0.5, 0.09375, ((0, 8), (1, 4)))
    after_up = centred(arg_keys[25], (D, FF), D ** -0.5, 0.09375, ((0, 8), (1, 4)))
    after_down = centred(arg_keys[26], (FF, D), FF ** -0.5, 0.0546875, ((0, 4), (1, 8)))
    return dict(block_in=block_in, before_gain=before_gain, before_gate=before_gate, before_up=before_up, before_down=before_down, mix_gain=mix_gain, input_gate=input_gate, input_value=input_value, input_write=input_write, input_read=input_read, input_step=input_step, step_bias=step_bias, decay_log=decay_log, skip_gain=skip_gain, value_taps=value_taps, write_taps=write_taps, read_taps=read_taps, value_window=value_window, write_window=write_window, read_window=read_window, scan_state=scan_state, group_gain=group_gain, mixer_out=mixer_out, after_gain=after_gain, after_gate=after_gate, after_up=after_up, after_down=after_down)


EPS = 1e-06

def half_channel(current, gain_vec, gate_weight, up_weight, down_weight):
    widened = current.astype(jnp.float32)
    row_scale = lax.rsqrt(lax.optimization_barrier(jnp.mean(widened * widened, axis=1, keepdims=True)) + EPS)
    lifted = (widened * gain_vec.astype(jnp.float32)).astype(jnp.bfloat16)
    gate_sum = jnp.dot(lifted, gate_weight, preferred_element_type=jnp.float32) * row_scale
    up_sum = jnp.dot(lifted, up_weight, preferred_element_type=jnp.float32) * row_scale
    hidden = (jax.nn.silu(gate_sum) * up_sum).astype(jnp.bfloat16)
    down_sum = jnp.dot(hidden, down_weight, preferred_element_type=jnp.float32)
    return (widened + 0.5 * down_sum).astype(jnp.bfloat16)

def short_conv(window_state, fresh, taps):
    window = jnp.concatenate([window_state, fresh[:, None, :]], axis=1)
    conv_sum = lax.optimization_barrier(jnp.sum(window.astype(jnp.float32) * taps.astype(jnp.float32)[None], axis=1))
    return (jax.nn.silu(conv_sum), window[:, 1:])

def spread_groups(vectors, heads):
    count = vectors.shape[0]
    groups = vectors.shape[1] // STATE
    shaped = vectors.reshape(count, groups, 1, STATE)
    return jnp.broadcast_to(shaped, (count, groups, heads // groups, STATE)).reshape(count, heads, STATE)

def state_update(gate_rows, value_conv, write_conv, read_conv, step_raw, step_bias, decay_log, skip_gain, scan_state):
    count = value_conv.shape[0]
    heads = step_bias.shape[0]
    step_size = jax.nn.softplus(step_raw + step_bias[None, :])
    decay = jnp.exp(-step_size * jnp.exp(decay_log)[None, :])
    value_heads = value_conv.reshape(count, heads, HEAD_DIM)
    write_heads = spread_groups(write_conv, heads)
    read_heads = spread_groups(read_conv, heads)
    state_next = decay[:, :, None, None] * scan_state + (step_size[:, :, None] * value_heads)[:, :, :, None] * write_heads[:, :, None, :]
    readout = lax.optimization_barrier(jnp.sum(state_next * read_heads[:, :, None, :], axis=3)) + skip_gain[None, :, None] * value_heads
    gated = readout.reshape(count, heads * HEAD_DIM) * jax.nn.silu(gate_rows.astype(jnp.float32))
    groups = write_conv.shape[1] // STATE
    grouped = gated.reshape(count, groups, heads * HEAD_DIM // groups)
    grouped = grouped * lax.rsqrt(lax.optimization_barrier(jnp.mean(grouped * grouped, axis=2, keepdims=True)) + EPS)
    return (grouped.reshape(count, heads * HEAD_DIM), state_next)

def reference(block_in, before_gain, before_gate, before_up, before_down, mix_gain, input_gate, input_value, input_write, input_read, input_step, step_bias, decay_log, skip_gain, value_taps, write_taps, read_taps, value_window, write_window, read_window, scan_state, group_gain, mixer_out, after_gain, after_gate, after_up, after_down):
    first_out = half_channel(block_in, before_gain, before_gate, before_up, before_down)
    widened = first_out.astype(jnp.float32)
    mix_scale = lax.rsqrt(lax.optimization_barrier(jnp.mean(widened * widened, axis=1, keepdims=True)) + EPS)
    lifted = (widened * mix_gain.astype(jnp.float32)).astype(jnp.bfloat16)
    gate_rows = (jnp.dot(lifted, input_gate, preferred_element_type=jnp.float32) * mix_scale).astype(jnp.bfloat16)
    value_fresh = (jnp.dot(lifted, input_value, preferred_element_type=jnp.float32) * mix_scale).astype(jnp.bfloat16)
    write_fresh = (jnp.dot(lifted, input_write, preferred_element_type=jnp.float32) * mix_scale).astype(jnp.bfloat16)
    read_fresh = (jnp.dot(lifted, input_read, preferred_element_type=jnp.float32) * mix_scale).astype(jnp.bfloat16)
    step_raw = jnp.dot(lifted, input_step, preferred_element_type=jnp.float32) * mix_scale
    value_conv, value_next = short_conv(value_window, value_fresh, value_taps)
    write_conv, write_next = short_conv(write_window, write_fresh, write_taps)
    read_conv, read_next = short_conv(read_window, read_fresh, read_taps)
    normed, state_next = state_update(gate_rows, value_conv, write_conv, read_conv, step_raw, step_bias, decay_log, skip_gain, scan_state)
    mixer_rows = (normed * group_gain.astype(jnp.float32)[None, :]).astype(jnp.bfloat16)
    middle = (widened + jnp.dot(mixer_rows, mixer_out, preferred_element_type=jnp.float32)).astype(jnp.bfloat16)
    block_out = half_channel(middle, after_gain, after_gate, after_up, after_down)
    return (block_out, state_next, value_next, write_next, read_next)
```

```python
import functools
from typing import Any, NamedTuple

import jax
import jax.numpy as jnp
from jax import lax
from jax.experimental import pallas as pl
from jax.experimental.pallas import tpu as pltpu
from jax.sharding import PartitionSpec as P

HEAD_DIM = 64
STATE = 128
EPS = 1e-06
TILE = 256
CHUNKS = 4
MIX_CHUNKS = 2
LANES = 128

MESH = pl.DeviceIdType.MESH
KV, TP = "kv", "tp"


class Geo(NamedTuple):
    n: int
    ny: int
    nz: int
    t: int
    nx: int
    cores: int


class At(NamedTuple):
    kv: Any
    z: Any
    y: Any
    tp: Any
    x: Any
    c: Any


def leading(line, key):
    keys = [key(d) for d in line]
    count = 1
    while count < len(keys) and keys[count] == keys[0]:
        count += 1
    return count if len(keys) % count == 0 else 1


def geometry(mesh):
    devices = mesh.devices
    n, t = mesh.shape[KV], mesh.shape[TP]
    if mesh.axis_names.index(KV) == 1:
        devices = devices.T
    ny = leading(devices[:, 0], lambda d: d.coords[2])
    cores = leading(devices[0], lambda d: tuple(d.coords))
    return Geo(n, ny, n // ny, t, t // cores, cores)


def place(geo):
    kv, tp = lax.axis_index(KV), lax.axis_index(TP)
    return At(kv, kv // geo.ny, lax.rem(kv, geo.ny), tp, tp // geo.cores, lax.rem(tp, geo.cores))


def sems(*shape):
    return pltpu.SemaphoreType.DMA(tuple(max(1, s) for s in shape))


def remote(src, dst, send_sem, recv_sem, axis, peer):
    return pltpu.make_async_remote_copy(
        src_ref=src,
        dst_ref=dst,
        send_sem=send_sem,
        recv_sem=recv_sem,
        device_id={axis: peer},
        device_id_type=MESH,
    )


def along_z(geo, z, k):
    if geo.nz & (geo.nz - 1):
        return lax.rem(z + k, geo.nz)
    bit = 1
    while bit < geo.nz:
        if k & bit:
            z = z + bit - 2 * bit * lax.rem(z // bit, 2)
        bit *= 2
    return z


def came_from(geo, z, k):
    return lax.rem(z + geo.nz - k, geo.nz) if geo.nz & (geo.nz - 1) else along_z(geo, z, k)


def hail(geo, at):
    barrier = pltpu.get_barrier_semaphore()
    for d in range(1, geo.t):
        peer = lax.rem(at.tp + d, geo.t)
        pl.semaphore_signal(barrier, inc=1, device_id={TP: peer}, device_id_type=MESH)
    for d in range(1, geo.ny):
        peer = at.z * geo.ny + lax.rem(at.y + d, geo.ny)
        pl.semaphore_signal(barrier, inc=1, device_id={KV: peer}, device_id_type=MESH)
    for e in range(1, geo.nz):
        peer = along_z(geo, at.z, e) * geo.ny + at.y
        pl.semaphore_signal(barrier, inc=1, device_id={KV: peer}, device_id_type=MESH)


def meet(geo):
    count = geo.t - 1 + geo.ny - 1 + geo.nz - 1
    pl.semaphore_wait(pltpu.get_barrier_semaphore(), count)


class SumRefs(NamedTuple):
    parts: Any
    staged: Any
    partial: Any
    landed: Any
    y_send: Any
    y_recv: Any
    z_send: Any
    z_recv: Any


def sum_refs(geo, block, width, dtype):
    across_y = (max(1, geo.ny - 1), geo.nz)
    along = (max(1, geo.nz - 1), block, width)
    return SumRefs(
        pltpu.VMEM((geo.ny, geo.nz, block, width), dtype),
        pltpu.VMEM(across_y + (block, width), dtype),
        pltpu.VMEM(along, dtype),
        pltpu.VMEM(along, dtype),
        sems(*across_y), sems(*across_y), sems(geo.nz - 1), sems(geo.nz - 1),
    )


class Scatter:
    def __init__(self, geo, at, refs):
        self.geo, self.at, self.refs = geo, at, refs
        self.parts, self.staged = refs.parts, refs.staged
        self.partial, self.landed = refs.partial, refs.landed
        self.first, self.second = {}, {}

    def put(self, i, columns, value):
        ny = self.geo.ny
        self.parts[i % ny, i // ny, :, columns] = value.astype(self.parts.dtype)

    def send(self):
        geo, at = self.geo, self.at
        for e in range(geo.nz - 1, -1, -1):
            zz = along_z(geo, at.z, e)
            for d in range(1, geo.ny):
                yy = lax.rem(at.y + d, geo.ny)
                copy = remote(
                    self.parts.at[yy, zz], self.staged.at[d - 1, e],
                    self.refs.y_send.at[d - 1, e], self.refs.y_recv.at[d - 1, e],
                    KV, at.z * geo.ny + yy,
                )
                copy.start()
                self.first[d, e] = copy

    def joined(self, e):
        geo, at = self.geo, self.at
        zz = along_z(geo, at.z, e)
        total = self.parts[at.y, zz].astype(jnp.float32)
        for d in range(1, geo.ny):
            self.first[d, e].wait_recv()
            total = total + self.staged[d - 1, e].astype(jnp.float32)
        return total, zz

    def relay(self):
        geo, at = self.geo, self.at
        for e in range(geo.nz - 1, 0, -1):
            total, zz = self.joined(e)
            self.partial[e - 1] = total.astype(self.partial.dtype)
            copy = remote(
                self.partial.at[e - 1], self.landed.at[e - 1],
                self.refs.z_send.at[e - 1], self.refs.z_recv.at[e - 1],
                KV, zz * geo.ny + at.y,
            )
            copy.start()
            self.second[e] = copy

    def collect(self):
        total, _ = self.joined(0)
        for e in range(self.geo.nz - 1, 0, -1):
            self.second[e].wait_recv()
            total = total + self.landed[e - 1].astype(jnp.float32)
        return total

    def drain(self):
        for copy in list(self.first.values()) + list(self.second.values()):
            copy.wait_send()


class RowRefs(NamedTuple):
    z_send: Any
    z_recv: Any
    y_send: Any
    y_recv: Any


def row_refs(geo):
    return RowRefs(
        sems(geo.nz - 1), sems(geo.nz - 1), sems(geo.ny - 1, geo.nz), sems(geo.ny - 1, geo.nz)
    )


class Gather:
    def __init__(self, geo, at, refs, rows):
        self.geo, self.at, self.refs, self.rows = geo, at, refs, rows
        self.first, self.second = {}, {}

    def pass_on(self, src, index, e):
        geo, at = self.geo, self.at
        for d in range(1, geo.ny):
            yy = lax.rem(at.y + d, geo.ny)
            copy = remote(
                src, self.rows.at[index],
                self.refs.y_send.at[d - 1, e], self.refs.y_recv.at[d - 1, e],
                KV, at.z * geo.ny + yy,
            )
            copy.start()
            self.second[d, e] = copy

    def start(self):
        geo, at = self.geo, self.at
        src = self.rows.at[at.kv]
        for e in range(geo.nz - 1, 0, -1):
            zz = along_z(geo, at.z, e)
            copy = remote(
                src, self.rows.at[at.kv], self.refs.z_send.at[e - 1], self.refs.z_recv.at[e - 1],
                KV, zz * geo.ny + at.y,
            )
            copy.start()
            self.first[e] = copy
        self.pass_on(src, at.kv, 0)

    def forward(self):
        geo, at = self.geo, self.at
        for e in range(1, geo.nz):
            self.first[e].wait_recv()
            index = came_from(geo, at.z, e) * geo.ny + at.y
            self.pass_on(self.rows.at[index], index, e)

    def finish(self):
        for copy in self.second.values():
            copy.wait_recv()

    def drain(self):
        for copy in list(self.first.values()) + list(self.second.values()):
            copy.wait_send()


def stacked(rows):
    n, block, width = rows.shape
    wide = rows[...].astype(jnp.float32).reshape(n * block, width)
    return wide.astype(rows.dtype)


class ReduceRefs(NamedTuple):
    terms: Any
    pair: Any
    mine: Any
    far: Any
    near_send: Any
    near_recv: Any
    far_send: Any
    far_recv: Any


def reduce_refs(geo, rows, width):
    half = rows // geo.cores
    across_x = (max(1, geo.nx - 1), geo.cores)
    return ReduceRefs(
        pltpu.VMEM((rows, width), jnp.float32),
        pltpu.VMEM((max(1, geo.cores - 1), rows, width), jnp.float32),
        pltpu.VMEM((geo.cores, half, width), jnp.bfloat16),
        pltpu.VMEM(across_x + (half, width), jnp.bfloat16),
        sems(geo.cores - 1), sems(geo.cores - 1), sems(*across_x), sems(*across_x),
    )


def reduce_rows(geo, at, r, base, weight, out):
    terms, pair, mine, far = r.terms, r.pair, r.mine, r.far
    sends = []
    for q in range(1, geo.cores):
        copy = remote(
            terms, pair.at[q - 1], r.near_send.at[q - 1], r.near_recv.at[q - 1],
            TP, at.x * geo.cores + lax.rem(at.c + q, geo.cores),
        )
        copy.start()
        sends.append(copy)
    half = mine.shape[1]
    for copy in sends:
        copy.wait_recv()
    for h in range(geo.cores):
        total = terms[h * half : (h + 1) * half]
        for q in range(1, geo.cores):
            total = total + pair[q - 1, h * half : (h + 1) * half]
        mine[h] = total.astype(mine.dtype)
    crossing = {}
    for dx in range(1, geo.nx):
        for q in range(geo.cores):
            copy = remote(
                mine.at[at.c], far.at[dx - 1, q],
                r.far_send.at[dx - 1, q], r.far_recv.at[dx - 1, q],
                TP, lax.rem(at.x + dx, geo.nx) * geo.cores + lax.rem(at.c + q, geo.cores),
            )
            copy.start()
            crossing[dx, q] = copy
    for q in range(geo.cores):
        h = lax.rem(at.c + geo.cores - q, geo.cores)
        total = mine[h].astype(jnp.float32)
        for dx in range(1, geo.nx):
            crossing[dx, q].wait_recv()
            total = total + far[dx - 1, q].astype(jnp.float32)
        out[h] = (base[h].astype(jnp.float32) + weight * total).astype(out.dtype)
    return sends + list(crossing.values())


def tiles_of(width):
    size = TILE if width % TILE == 0 else 128
    return size, width // size


def chunk_widths(width):
    size, count = tiles_of(width)
    chunks = min(CHUNKS, count)
    return [size * (count // chunks + (k < count % chunks)) for k in range(chunks)]


def spread(scatter, lifted, weight, start, width, offset, n):
    size, count = tiles_of(width)
    block = lifted.shape[0] // n
    for k in range(count):
        tile = jnp.dot(
            lifted[...], weight[:, start + k * size : start + (k + 1) * size],
            preferred_element_type=jnp.float32,
        )
        columns = slice(offset + k * size, offset + (k + 1) * size)
        for i in range(n):
            scatter.put(i, columns, tile[i * block : (i + 1) * block])


def across(gain):
    wide = gain[...].astype(jnp.float32)
    return jnp.concatenate([wide[k : k + 1] for k in range(wide.shape[0])], axis=1)


def lift(geo, r, full, gain, aux):
    r.lifted[...] = (full * across(gain)).astype(jnp.bfloat16)
    squares = jnp.sum(full * full, axis=1, keepdims=True)
    block = full.shape[0] // geo.n
    for i in range(geo.n):
        part = squares[i * block : (i + 1) * block]
        aux.put(i, slice(0, 128), jnp.broadcast_to(part, (block, 128)))


class ChannelRefs(NamedTuple):
    lifted: Any
    squares: Any
    sums: Any
    hidden: Any
    passing: Any


def channel_refs(geo, rows, width, hidden):
    block = rows // geo.n
    widths = chunk_widths(hidden)
    return ChannelRefs(
        pltpu.VMEM((rows, width), jnp.bfloat16),
        sum_refs(geo, block, LANES, jnp.float32),
        [sum_refs(geo, block, 2 * columns, jnp.bfloat16) for columns in widths],
        [pltpu.VMEM((geo.n, block, columns), jnp.bfloat16) for columns in widths],
        [row_refs(geo) for _ in widths],
    )


def channel(geo, at, r, full, gain, loads, weights):
    rows, width = full.shape
    widths = chunk_widths(weights.gate.shape[1])
    squares = Scatter(geo, at, r.squares)
    lift(geo, r, full, gain, squares)
    squares.send()
    loads.gate.wait()
    loads.up.wait()
    scatters, gathers = [], []
    start = 0
    for k, columns in enumerate(widths):
        scatter = Scatter(geo, at, r.sums[k])
        spread(scatter, r.lifted, weights.gate, start, columns, 0, geo.n)
        spread(scatter, r.lifted, weights.up, start, columns, columns, geo.n)
        scatter.send()
        scatters.append(scatter)
        start += columns
    squares.relay()
    for scatter in scatters:
        scatter.relay()
    scale = lax.rsqrt(squares.collect()[:, :1] / (width * geo.n) + EPS)
    for k, columns in enumerate(widths):
        sums = scatters[k].collect() * scale
        gate_sum, up_sum = sums[:, :columns], sums[:, columns:]
        gather = Gather(geo, at, r.passing[k], r.hidden[k])
        hidden = gate_sum / (1.0 + jnp.exp(-gate_sum)) * up_sum
        gather.rows[at.kv] = hidden.astype(gather.rows.dtype)
        gather.start()
        if gathers:
            gathers[-1].forward()
        gathers.append(gather)
    gathers[-1].forward()
    loads.down.wait()
    total, start = None, 0
    for gather, columns in zip(gathers, widths):
        gather.finish()
        term = jnp.dot(
            stacked(gather.rows), weights.down[start : start + columns, :], preferred_element_type=jnp.float32
        )
        total = term if total is None else total + term
        start += columns
    return total, [squares] + scatters + gathers


def start_loads(arrays, places, loading):
    copies = []
    for k, (src, dst) in enumerate(zip(arrays, places)):
        copies.append(pltpu.make_async_copy(src, dst, loading.at[k]))
        copies[-1].start()
    return type(places)(*copies)


def resting(arrays):
    return type(arrays)(*(pltpu.VMEM(a.shape, a.dtype) for a in arrays))


def whole(ref):
    cores, half, width = ref.shape
    return ref[...].astype(jnp.float32).reshape(cores * half, width)


class FirstArrays(NamedTuple):
    own: Any
    before_gain: Any
    gate: Any
    up: Any
    down: Any
    mix_gain: Any
    in_step: Any
    in_value: Any
    in_write: Any
    in_read: Any
    in_gate: Any
    step_bias: Any
    decay_log: Any
    skip_gain: Any
    group_gain: Any
    value_taps: Any
    write_taps: Any
    read_taps: Any
    value_window: Any
    write_window: Any
    read_window: Any
    scan: Any


class FirstRefs(NamedTuple):
    held: Any
    loading: Any
    pieces: Any
    piece_send: Any
    piece_recv: Any
    base: Any
    channel: Any
    reduce: Any
    aux: Any
    mixed: Any
    gates: Any
    pushes: Any
    decays: Any
    pushed: Any
    both: Any
    passing: Any


def first_kernel(geo, tree, mixes, *refs):
    count = len(FirstArrays._fields)
    sources, refs = refs[:count], refs[count:]
    first_out, state, value_next, write_next, read_next = refs[:5]
    mixed_rows, refs = refs[5 : 5 + len(mixes)], refs[5 + len(mixes) :]
    r = jax.tree.unflatten(tree, refs)
    at = place(geo)
    held = FirstArrays(*r.held, state)
    loads = start_loads(sources, held, r.loading)
    hail(geo, at)
    meet(geo)
    pieces = r.pieces
    own = held.own
    loads.own.wait()
    moves = []
    for d in range(1, geo.t):
        copy = remote(
            own, pieces.at[at.tp], r.piece_send.at[d - 1], r.piece_recv.at[d - 1],
            TP, lax.rem(at.tp + d, geo.t),
        )
        copy.start()
        moves.append(copy)
    pieces[at.tp] = own[...]
    loads.before_gain.wait()
    for copy in moves:
        copy.wait_recv()
    full = jnp.concatenate([pieces[k].astype(jnp.float32) for k in range(geo.t)], axis=1)
    base = r.base
    half = base.shape[1]
    for h in range(geo.cores):
        base[h] = full[h * half : (h + 1) * half].astype(base.dtype)
    total, pending = channel(geo, at, r.channel, full, held.before_gain, loads, held)
    r.reduce.terms[...] = total
    moves += reduce_rows(geo, at, r.reduce, base, 0.5, first_out)
    features = full.shape[1] * geo.n
    aux = Scatter(geo, at, r.aux)
    loads.mix_gain.wait()
    lift(geo, r.channel, whole(first_out), held.mix_gain, aux)
    lifted = r.channel.lifted
    block = lifted.shape[0] // geo.n
    loads.in_step.wait()
    step = lax.dot_general(
        lifted[...], held.in_step[...], (((1,), (1,)), ((), ())),
        preferred_element_type=jnp.float32,
    )
    for i in range(geo.n):
        aux.put(i, slice(LANES, LANES + step.shape[1]), step[i * block : (i + 1) * block])
    aux.send()
    mixed = Scatter(geo, at, r.mixed)
    offset = 0
    for load, weight in zip(loads[7:10], held[7:10]):
        load.wait()
        spread(mixed, lifted, weight, 0, weight.shape[1], offset, geo.n)
        offset += weight.shape[1]
    mixed.send()
    gates = Scatter(geo, at, r.gates)
    loads.in_gate.wait()
    spread(gates, lifted, held.in_gate, 0, held.in_gate.shape[1], 0, geo.n)
    gates.send()
    for scatter in (aux, mixed, gates):
        scatter.relay()
    for load in loads[11:]:
        load.wait()
    aux_sum = aux.collect()
    scale = lax.rsqrt(aux_sum[:, :1] / features + EPS)
    tables = prepare(r, held, aux_sum, scale, mixed.collect(), value_next, write_next, read_next)
    group, gate_rows, gathers = 0, None, []
    for k, rows in enumerate(mixed_rows):
        gather = Gather(geo, at, r.passing[k], rows)
        span = rows.shape[2] // mixes[k]
        for j in range(mixes[k]):
            readout = advance(r, tables, state, group)
            if gate_rows is None:
                gate_rows = (gates.collect() * scale).astype(jnp.bfloat16).astype(jnp.float32)
            columns = slice(group * span, (group + 1) * span)
            part = (readout + tables.direct[:, columns]) * silu(gate_rows[:, columns])
            mean = jnp.mean(part * part, axis=1, keepdims=True)
            part = part * lax.rsqrt(mean + EPS) * tables.gain[:, columns]
            rows[at.kv, :, j * span : (j + 1) * span] = part.astype(rows.dtype)
            group += 1
        gather.start()
        gathers.append(gather)
    for gather in gathers:
        gather.forward()
    for gather in gathers:
        gather.finish()
    for copy in moves:
        copy.wait_send()
    for part in pending + [aux, mixed, gates] + gathers:
        part.drain()


class LastArrays(NamedTuple):
    gate: Any
    up: Any
    down: Any


class LastRefs(NamedTuple):
    held: Any
    loading: Any
    middle: Any
    channel: Any
    reduce: Any
    shares: Any
    kept: Any
    given: Any
    taken: Any
    end_send: Any
    end_recv: Any


def last_kernel(geo, tree, mixes, *refs):
    mixed_rows, refs = refs[: len(mixes)], refs[len(mixes) :]
    first_out, after_gain, out_weight = refs[:3]
    count = len(LastArrays._fields)
    sources, refs = refs[3 : 3 + count], refs[3 + count :]
    block_out = refs[0]
    r = jax.tree.unflatten(tree, refs[1:])
    at = place(geo)
    loads = start_loads(sources, r.held, r.loading)
    hail(geo, at)
    total, start = None, 0
    for rows in mixed_rows:
        stop = start + rows.shape[2]
        term = jnp.dot(
            stacked(rows), out_weight[start:stop, :], preferred_element_type=jnp.float32
        )
        total = term if total is None else total + term
        start = stop
    r.reduce.terms[...] = total
    meet(geo)
    middle = r.middle
    moves = reduce_rows(geo, at, r.reduce, first_out, 1.0, middle)
    full = whole(middle)
    width = block_out.shape[1]
    for k in range(geo.t):
        r.shares[k] = full[:, k * width : (k + 1) * width].astype(middle.dtype)
    total, pending = channel(geo, at, r.channel, full, after_gain, loads, r.held)
    for k in range(geo.t):
        part = total[:, k * width : (k + 1) * width]
        r.kept[k] = part
        r.given[k] = part.astype(jnp.bfloat16)
    ends = []
    for d in range(1, geo.t):
        peer = lax.rem(at.tp + d, geo.t)
        copy = remote(
            r.given.at[peer], r.taken.at[d - 1], r.end_send.at[d - 1], r.end_recv.at[d - 1],
            TP, peer,
        )
        copy.start()
        ends.append(copy)
    result = r.kept[at.tp]
    for d in range(1, geo.t):
        ends[d - 1].wait_recv()
        result = result + r.taken[d - 1].astype(jnp.float32)
    rest = r.shares[at.tp].astype(jnp.float32)
    block_out[...] = (rest + 0.5 * result).astype(block_out.dtype)
    for copy in moves + ends:
        copy.wait_send()
    for part in pending:
        part.drain()


def silu(v):
    return v / (1.0 + jnp.exp(-v))


def conv(window, fresh, taps, following):
    count = window.shape[0]
    wide = fresh.astype(jnp.float32)
    total = wide * taps[count : count + 1, :].astype(jnp.float32)
    for k in range(count):
        row = window[k]
        total = total + row.astype(jnp.float32) * taps[k : k + 1, :].astype(jnp.float32)
        if k:
            following[k - 1] = row
    following[count - 1] = fresh
    return silu(total)


def split(v):
    high = v.astype(jnp.bfloat16)
    return high, (v - high.astype(jnp.float32)).astype(jnp.bfloat16)


class Tables(NamedTuple):
    pushes: Any
    decays: Any
    write: Any
    read: Any
    direct: Any
    gain: Any


def prepare(r, held, aux_sum, scale, mixed_sum, value_next, write_next, read_next):
    block, heads = mixed_sum.shape[0], held.step_bias.shape[1]
    inner, vectors = value_next.shape[2], write_next.shape[2]
    fresh = (mixed_sum * scale).astype(jnp.bfloat16)
    value = conv(held.value_window, fresh[:, :inner], held.value_taps, value_next)
    write = conv(
        held.write_window, fresh[:, inner : inner + vectors], held.write_taps, write_next
    )
    read = conv(held.read_window, fresh[:, inner + vectors :], held.read_taps, read_next)
    raw = aux_sum[:, LANES : LANES + heads] * scale + held.step_bias[...]
    size = jnp.maximum(raw, 0.0) + jnp.log1p(jnp.exp(-jnp.abs(raw)))
    decay = jnp.exp(-size * jnp.exp(held.decay_log[...]))
    lane = lax.broadcasted_iota(jnp.int32, (1, 2 * HEAD_DIM), 1)

    def per_channel(v):
        return jnp.concatenate(
            [
                jnp.where(lane < HEAD_DIM, v[:, k : k + 1], v[:, k + 1 : k + 2])
                for k in range(0, heads, 2)
            ],
            axis=1,
        )

    high, low = split(value * per_channel(size))
    wide = high.astype(jnp.float32)
    pushes = jnp.concatenate([wide, wide, low.astype(jnp.float32)], axis=0)
    r.pushes[...] = pushes.T.astype(jnp.bfloat16)
    for h in range(heads):
        r.decays[h] = jnp.broadcast_to(decay[:, h : h + 1], (block, STATE))
    return Tables(
        r.pushes, r.decays, write, read,
        value * per_channel(held.skip_gain[...]), across(held.group_gain),
    )


def advance(r, tables, state, group):
    block, heads = state.shape[0], state.shape[1]
    per_group = heads // (tables.write.shape[1] // STATE)
    span = per_group * HEAD_DIM
    near = slice(group * STATE, (group + 1) * STATE)
    row = lax.broadcasted_iota(jnp.int32, (3 * block, STATE), 0)
    high, low = split(tables.write[:, near])
    wide = high.astype(jnp.float32)
    stack = jnp.concatenate([wide, low.astype(jnp.float32), wide], axis=0)
    writes = jnp.concatenate(
        [jnp.where(lax.rem(row, block) == b, stack, 0.0) for b in range(block)], axis=1
    ).astype(jnp.bfloat16)
    pushed, both = r.pushed, r.both
    pushed[...] = jnp.dot(
        tables.pushes[group * span : (group + 1) * span, :], writes,
        preferred_element_type=jnp.float32,
    )
    reads = jnp.concatenate(
        [v.astype(jnp.float32) for v in split(tables.read[:, near])], axis=0
    ).T
    lane = lax.broadcasted_iota(jnp.int32, reads.shape, 1)
    picks = []
    for b in range(block):
        pick = jnp.where(lax.rem(lane, block) == b, reads, 0.0).astype(jnp.bfloat16)
        picks += [pick, pick]
        for j in range(per_group):
            h = group * per_group + j
            spot = slice(j * HEAD_DIM, (j + 1) * HEAD_DIM)
            fresh = tables.decays[h, b : b + 1, :] * state[b, h]
            fresh = fresh + pushed[spot, b * STATE : (b + 1) * STATE]
            state[b, h] = fresh
            high, low = split(fresh)
            both[spot, 2 * b * STATE : (2 * b + 1) * STATE] = high
            both[spot, (2 * b + 1) * STATE : (2 * b + 2) * STATE] = low
    seen = jnp.dot(
        both[...], jnp.concatenate(picks, axis=0), preferred_element_type=jnp.float32
    ).T
    return seen[:block] + seen[block:]


VMEM = pl.BlockSpec(memory_space=pltpu.VMEM)
HBM = pl.BlockSpec(memory_space=pltpu.HBM)


def communicate(kernel, near, far, outs, scratch, ident, limit, micros):
    return pl.pallas_call(
        kernel,
        out_shape=outs,
        in_specs=[VMEM] * len(near) + [HBM] * len(far),
        out_specs=jax.tree.map(lambda _: VMEM, outs),
        scratch_shapes=scratch,
        compiler_params=pltpu.CompilerParams(
            collective_id=ident, has_side_effects=True, vmem_limit_bytes=limit
        ),
        cost_estimate=pl.CostEstimate(
            flops=0, bytes_accessed=micros * 3_000_000, transcendentals=0
        ),
    )(*near, *far)


def mix_groups(groups):
    chunks = min(MIX_CHUNKS, groups)
    return [groups // chunks + (k < groups % chunks) for k in range(chunks)]


def first_call(geo, by):
    shape = jax.ShapeDtypeStruct
    rows, width = by.own.shape[0], by.gate.shape[0]
    block = rows // geo.n
    inner, vectors = by.in_value.shape[1], by.in_write.shape[1]
    groups, heads = vectors // STATE, by.scan.shape[1]
    mixes = mix_groups(groups)
    span = inner // groups
    scratch = FirstRefs(
        tuple(resting(by))[:-1],
        sems(len(by)),
        pltpu.VMEM((geo.t,) + by.own.shape, by.own.dtype),
        sems(geo.t - 1), sems(geo.t - 1),
        pltpu.VMEM((geo.cores, rows // geo.cores, width), by.own.dtype),
        channel_refs(geo, rows, width, by.gate.shape[1]),
        reduce_refs(geo, rows, width),
        sum_refs(geo, block, LANES + by.in_step.shape[0], jnp.float32),
        sum_refs(geo, block, inner + 2 * vectors, jnp.bfloat16),
        sum_refs(geo, block, inner, jnp.bfloat16),
        pltpu.VMEM((inner, 3 * block), jnp.bfloat16),
        pltpu.VMEM((heads, block, STATE), jnp.float32),
        pltpu.VMEM((span, block * STATE), jnp.float32),
        pltpu.VMEM((span, 2 * block * STATE), jnp.bfloat16),
        [row_refs(geo) for _ in mixes],
    )
    leaves, tree = jax.tree.flatten(scratch)
    windows = (by.value_window, by.write_window, by.read_window)
    outs = (
        shape((geo.cores, rows // geo.cores, width), jnp.bfloat16),
        shape(by.scan.shape, by.scan.dtype),
        *(shape(w.shape, w.dtype) for w in windows),
        *(shape((geo.n, block, k * span), jnp.bfloat16) for k in mixes),
    )
    kernel = functools.partial(first_kernel, geo, tree, mixes)
    return mixes, communicate(kernel, (), by, outs, leaves, 0, 44 * 2**20, 50)


def last_call(geo, mixes, mixed_rows, first_out, after_gain, mixer_out, weights, share):
    rows = first_out.shape[0] * first_out.shape[1]
    width, hidden = weights.gate.shape
    scratch = LastRefs(
        resting(weights),
        sems(len(weights)),
        pltpu.VMEM(first_out.shape, first_out.dtype),
        channel_refs(geo, rows, width, hidden),
        reduce_refs(geo, rows, width),
        pltpu.VMEM((geo.t, rows, share), jnp.bfloat16),
        pltpu.VMEM((geo.t, rows, share), jnp.float32),
        pltpu.VMEM((geo.t, rows, share), jnp.bfloat16),
        pltpu.VMEM((max(1, geo.t - 1), rows, share), jnp.bfloat16),
        sems(geo.t - 1), sems(geo.t - 1),
    )
    leaves, tree = jax.tree.flatten(scratch)
    return communicate(
        functools.partial(last_kernel, geo, tree, mixes),
        (*mixed_rows, first_out, after_gain, mixer_out), weights,
        jax.ShapeDtypeStruct((rows, share), jnp.bfloat16), leaves, 1, 24 * 2**20, 36,
    )


def deliver_kernel(*refs):
    count = len(refs) // 2
    sems = refs[-1]
    copies = []
    for k in range(count):
        copy = pltpu.make_async_copy(refs[k], refs[count + k], sems.at[k])
        copy.start()
        copies.append(copy)
    for copy in copies:
        copy.wait()


def deliver(*arrays):
    return pl.pallas_call(
        deliver_kernel,
        out_shape=tuple(jax.ShapeDtypeStruct(a.shape, a.dtype) for a in arrays),
        in_specs=[VMEM] * len(arrays),
        out_specs=[HBM] * len(arrays),
        scratch_shapes=[pltpu.SemaphoreType.DMA((len(arrays),))],
        compiler_params=pltpu.CompilerParams(vmem_limit_bytes=12 * 2**20),
    )(*arrays)


def stay(arrays):
    return type(arrays)(*(pltpu.with_memory_space_constraint(a, pltpu.HBM) for a in arrays))


def local(
    geo,
    block_in,
    before_gain,
    before_gate,
    before_up,
    before_down,
    mix_gain,
    input_gate,
    input_value,
    input_write,
    input_read,
    input_step,
    step_bias,
    decay_log,
    skip_gain,
    value_taps,
    write_taps,
    read_taps,
    value_window,
    write_window,
    read_window,
    scan_state,
    group_gain,
    mixer_out,
    after_gain,
    after_gate,
    after_up,
    after_down,
):
    def line(vector):
        return vector.reshape(1, -1)

    def lanes(vector):
        return vector.reshape(-1, LANES)

    windows = [w.transpose(1, 0, 2) for w in (value_window, write_window, read_window)]
    mixes, (first_out, state_next, value_next, write_next, read_next, *mixed_rows) = first_call(
        geo,
        stay(FirstArrays(
            block_in, lanes(before_gain), before_gate, before_up, before_down, lanes(mix_gain),
            input_step.T, input_value, input_write, input_read, input_gate,
            line(step_bias), line(decay_log), line(skip_gain), lanes(group_gain),
            value_taps, write_taps, read_taps, *windows, scan_state,
        )),
    )
    block_out = last_call(
        geo, mixes, mixed_rows, first_out, lanes(after_gain), mixer_out,
        stay(LastArrays(after_gate, after_up, after_down)), block_in.shape[1],
    )
    block_out, state_next, *following = deliver(
        block_out, state_next, value_next, write_next, read_next
    )
    return (block_out, state_next, *(w.transpose(1, 0, 2) for w in following))


def solution(mesh):
    placed = (
        P(None, (KV, TP)),
        P(KV),
        P(KV, TP),
        P(KV, TP),
        P(TP, KV),
        P(KV),
        P(KV, TP),
        P(KV, TP),
        P(KV, TP),
        P(KV, TP),
        P(KV, TP),
        P(TP),
        P(TP),
        P(TP),
        P(None, TP),
        P(None, TP),
        P(None, TP),
        P(KV, None, TP),
        P(KV, None, TP),
        P(KV, None, TP),
        P(KV, TP, None, None),
        P(TP),
        P(TP, KV),
        P(KV),
        P(KV, TP),
        P(KV, TP),
        P(TP, KV),
    )
    return jax.shard_map(
        functools.partial(local, geometry(mesh)),
        mesh=mesh,
        in_specs=placed,
        out_specs=(
            P(None, (KV, TP)),
            P(KV, TP, None, None),
            P(KV, None, TP),
            P(KV, None, TP),
            P(KV, None, TP),
        ),
        check_vma=False,
    )
```

```python
import functools
from typing import Any, NamedTuple

import jax
import jax.numpy as jnp
from jax import lax
from jax.experimental import pallas as pl
from jax.experimental.pallas import tpu as pltpu
from jax.sharding import PartitionSpec as P

HEAD_DIM = 64
STATE = 128
EPS = 1e-06
TILE = 256
CHUNKS = 4
MIX_CHUNKS = 2
LANES = 128

MESH = pl.DeviceIdType.MESH
KV, TP = "kv", "tp"


class Geo(NamedTuple):
    n: int
    ny: int
    nz: int
    t: int
    nx: int
    cores: int


class At(NamedTuple):
    kv: Any
    z: Any
    y: Any
    tp: Any
    x: Any
    c: Any


def leading(line, key):
    keys = [key(d) for d in line]
    count = 1
    while count < len(keys) and keys[count] == keys[0]:
        count += 1
    return count if len(keys) % count == 0 else 1


def geometry(mesh):
    devices = mesh.devices
    n, t = mesh.shape[KV], mesh.shape[TP]
    if mesh.axis_names.index(KV) == 1:
        devices = devices.T
    ny = leading(devices[:, 0], lambda d: d.coords[2])
    cores = leading(devices[0], lambda d: tuple(d.coords))
    return Geo(n, ny, n // ny, t, t // cores, cores)


def place(geo):
    kv, tp = lax.axis_index(KV), lax.axis_index(TP)
    return At(kv, kv // geo.ny, lax.rem(kv, geo.ny), tp, tp // geo.cores, lax.rem(tp, geo.cores))


def sems(*shape):
    return pltpu.SemaphoreType.DMA(tuple(max(1, s) for s in shape))


def remote(src, dst, send_sem, recv_sem, axis, peer):
    return pltpu.make_async_remote_copy(
        src_ref=src,
        dst_ref=dst,
        send_sem=send_sem,
        recv_sem=recv_sem,
        device_id={axis: peer},
        device_id_type=MESH,
    )


def along_z(geo, z, k):
    if geo.nz & (geo.nz - 1):
        return lax.rem(z + k, geo.nz)
    bit = 1
    while bit < geo.nz:
        if k & bit:
            z = z + bit - 2 * bit * lax.rem(z // bit, 2)
        bit *= 2
    return z


def came_from(geo, z, k):
    return lax.rem(z + geo.nz - k, geo.nz) if geo.nz & (geo.nz - 1) else along_z(geo, z, k)


def hail(geo, at):
    barrier = pltpu.get_barrier_semaphore()
    for d in range(1, geo.t):
        peer = lax.rem(at.tp + d, geo.t)
        pl.semaphore_signal(barrier, inc=1, device_id={TP: peer}, device_id_type=MESH)
    for d in range(1, geo.ny):
        peer = at.z * geo.ny + lax.rem(at.y + d, geo.ny)
        pl.semaphore_signal(barrier, inc=1, device_id={KV: peer}, device_id_type=MESH)
    for e in range(1, geo.nz):
        peer = along_z(geo, at.z, e) * geo.ny + at.y
        pl.semaphore_signal(barrier, inc=1, device_id={KV: peer}, device_id_type=MESH)


def meet(geo):
    count = geo.t - 1 + geo.ny - 1 + geo.nz - 1
    pl.semaphore_wait(pltpu.get_barrier_semaphore(), count)


class SumRefs(NamedTuple):
    parts: Any
    staged: Any
    partial: Any
    landed: Any
    y_send: Any
    y_recv: Any
    z_send: Any
    z_recv: Any


def sum_refs(geo, block, width, dtype):
    across_y = (max(1, geo.ny - 1), geo.nz)
    along = (max(1, geo.nz - 1), block, width)
    return SumRefs(
        pltpu.VMEM((geo.ny, geo.nz, block, width), dtype),
        pltpu.VMEM(across_y + (block, width), dtype),
        pltpu.VMEM(along, dtype),
        pltpu.VMEM(along, dtype),
        sems(*across_y), sems(*across_y), sems(geo.nz - 1), sems(geo.nz - 1),
    )


class Scatter:
    def __init__(self, geo, at, refs):
        self.geo, self.at, self.refs = geo, at, refs
        self.parts, self.staged = refs.parts, refs.staged
        self.partial, self.landed = refs.partial, refs.landed
        self.first, self.second = {}, {}

    def put(self, i, columns, value):
        ny = self.geo.ny
        self.parts[i % ny, i // ny, :, columns] = value.astype(self.parts.dtype)

    def send(self):
        geo, at = self.geo, self.at
        for e in range(geo.nz - 1, -1, -1):
            zz = along_z(geo, at.z, e)
            for d in range(1, geo.ny):
                yy = lax.rem(at.y + d, geo.ny)
                copy = remote(
                    self.parts.at[yy, zz], self.staged.at[d - 1, e],
                    self.refs.y_send.at[d - 1, e], self.refs.y_recv.at[d - 1, e],
                    KV, at.z * geo.ny + yy,
                )
                copy.start()
                self.first[d, e] = copy

    def joined(self, e):
        geo, at = self.geo, self.at
        zz = along_z(geo, at.z, e)
        total = self.parts[at.y, zz].astype(jnp.float32)
        for d in range(1, geo.ny):
            self.first[d, e].wait_recv()
            total = total + self.staged[d - 1, e].astype(jnp.float32)
        return total, zz

    def relay(self):
        geo, at = self.geo, self.at
        for e in range(geo.nz - 1, 0, -1):
            total, zz = self.joined(e)
            self.partial[e - 1] = total.astype(self.partial.dtype)
            copy = remote(
                self.partial.at[e - 1], self.landed.at[e - 1],
                self.refs.z_send.at[e - 1], self.refs.z_recv.at[e - 1],
                KV, zz * geo.ny + at.y,
            )
            copy.start()
            self.second[e] = copy

    def collect(self):
        total, _ = self.joined(0)
        for e in range(self.geo.nz - 1, 0, -1):
            self.second[e].wait_recv()
            total = total + self.landed[e - 1].astype(jnp.float32)
        return total

    def drain(self):
        for copy in list(self.first.values()) + list(self.second.values()):
            copy.wait_send()


class RowRefs(NamedTuple):
    z_send: Any
    z_recv: Any
    y_send: Any
    y_recv: Any


def row_refs(geo):
    return RowRefs(
        sems(geo.nz - 1), sems(geo.nz - 1), sems(geo.ny - 1, geo.nz), sems(geo.ny - 1, geo.nz)
    )


class Gather:
    def __init__(self, geo, at, refs, rows):
        self.geo, self.at, self.refs, self.rows = geo, at, refs, rows
        self.first, self.second = {}, {}

    def pass_on(self, src, index, e):
        geo, at = self.geo, self.at
        for d in range(1, geo.ny):
            yy = lax.rem(at.y + d, geo.ny)
            copy = remote(
                src, self.rows.at[index],
                self.refs.y_send.at[d - 1, e], self.refs.y_recv.at[d - 1, e],
                KV, at.z * geo.ny + yy,
            )
            copy.start()
            self.second[d, e] = copy

    def start(self):
        geo, at = self.geo, self.at
        src = self.rows.at[at.kv]
        for e in range(geo.nz - 1, 0, -1):
            zz = along_z(geo, at.z, e)
            copy = remote(
                src, self.rows.at[at.kv], self.refs.z_send.at[e - 1], self.refs.z_recv.at[e - 1],
                KV, zz * geo.ny + at.y,
            )
            copy.start()
            self.first[e] = copy
        self.pass_on(src, at.kv, 0)

    def forward(self):
        geo, at = self.geo, self.at
        for e in range(1, geo.nz):
            self.first[e].wait_recv()
            index = came_from(geo, at.z, e) * geo.ny + at.y
            self.pass_on(self.rows.at[index], index, e)

    def finish(self):
        for copy in self.second.values():
            copy.wait_recv()

    def drain(self):
        for copy in list(self.first.values()) + list(self.second.values()):
            copy.wait_send()


def stacked(rows):
    n, block, width = rows.shape
    wide = rows[...].astype(jnp.float32).reshape(n * block, width)
    return wide.astype(rows.dtype)


class ReduceRefs(NamedTuple):
    terms: Any
    pair: Any
    mine: Any
    far: Any
    near_send: Any
    near_recv: Any
    far_send: Any
    far_recv: Any


def reduce_refs(geo, rows, width):
    half = rows // geo.cores
    across_x = (max(1, geo.nx - 1), geo.cores)
    return ReduceRefs(
        pltpu.VMEM((rows, width), jnp.float32),
        pltpu.VMEM((max(1, geo.cores - 1), rows, width), jnp.float32),
        pltpu.VMEM((geo.cores, half, width), jnp.bfloat16),
        pltpu.VMEM(across_x + (half, width), jnp.bfloat16),
        sems(geo.cores - 1), sems(geo.cores - 1), sems(*across_x), sems(*across_x),
    )


def reduce_rows(geo, at, r, base, weight, out):
    terms, pair, mine, far = r.terms, r.pair, r.mine, r.far
    sends = []
    for q in range(1, geo.cores):
        copy = remote(
            terms, pair.at[q - 1], r.near_send.at[q - 1], r.near_recv.at[q - 1],
            TP, at.x * geo.cores + lax.rem(at.c + q, geo.cores),
        )
        copy.start()
        sends.append(copy)
    half = mine.shape[1]
    for copy in sends:
        copy.wait_recv()
    for h in range(geo.cores):
        total = terms[h * half : (h + 1) * half]
        for q in range(1, geo.cores):
            total = total + pair[q - 1, h * half : (h + 1) * half]
        mine[h] = total.astype(mine.dtype)
    crossing = {}
    for dx in range(1, geo.nx):
        for q in range(geo.cores):
            copy = remote(
                mine.at[at.c], far.at[dx - 1, q],
                r.far_send.at[dx - 1, q], r.far_recv.at[dx - 1, q],
                TP, lax.rem(at.x + dx, geo.nx) * geo.cores + lax.rem(at.c + q, geo.cores),
            )
            copy.start()
            crossing[dx, q] = copy
    for q in range(geo.cores):
        h = lax.rem(at.c + geo.cores - q, geo.cores)
        total = mine[h].astype(jnp.float32)
        for dx in range(1, geo.nx):
            crossing[dx, q].wait_recv()
            total = total + far[dx - 1, q].astype(jnp.float32)
        out[h] = (base[h].astype(jnp.float32) + weight * total).astype(out.dtype)
    return sends + list(crossing.values())


def tiles_of(width):
    size = TILE if width % TILE == 0 else 128
    return size, width // size


def chunk_widths(width):
    size, count = tiles_of(width)
    chunks = min(CHUNKS, count)
    return [size * (count // chunks + (k < count % chunks)) for k in range(chunks)]


def spread(scatter, lifted, weight, start, width, offset, n):
    size, count = tiles_of(width)
    block = lifted.shape[0] // n
    for k in range(count):
        tile = jnp.dot(
            lifted[...], weight[:, start + k * size : start + (k + 1) * size],
            preferred_element_type=jnp.float32,
        )
        columns = slice(offset + k * size, offset + (k + 1) * size)
        for i in range(n):
            scatter.put(i, columns, tile[i * block : (i + 1) * block])


def across(gain):
    wide = gain[...].astype(jnp.float32)
    return jnp.concatenate([wide[k : k + 1] for k in range(wide.shape[0])], axis=1)


def lift(geo, r, full, gain, aux):
    r.lifted[...] = (full * across(gain)).astype(jnp.bfloat16)
    squares = jnp.sum(full * full, axis=1, keepdims=True)
    block = full.shape[0] // geo.n
    for i in range(geo.n):
        part = squares[i * block : (i + 1) * block]
        aux.put(i, slice(0, 128), jnp.broadcast_to(part, (block, 128)))


class ChannelRefs(NamedTuple):
    lifted: Any
    squares: Any
    sums: Any
    hidden: Any
    passing: Any


def channel_refs(geo, rows, width, hidden):
    block = rows // geo.n
    widths = chunk_widths(hidden)
    return ChannelRefs(
        pltpu.VMEM((rows, width), jnp.bfloat16),
        sum_refs(geo, block, LANES, jnp.float32),
        [sum_refs(geo, block, 2 * columns, jnp.bfloat16) for columns in widths],
        [pltpu.VMEM((geo.n, block, columns), jnp.bfloat16) for columns in widths],
        [row_refs(geo) for _ in widths],
    )


def channel(geo, at, r, full, gain, loads, weights, meanwhile=None):
    rows, width = full.shape
    widths = chunk_widths(weights.gate.shape[1])
    squares = Scatter(geo, at, r.squares)
    lift(geo, r, full, gain, squares)
    squares.send()
    loads.gate.wait()
    loads.up.wait()
    scatters, gathers = [], []
    start = 0
    for k, columns in enumerate(widths):
        scatter = Scatter(geo, at, r.sums[k])
        spread(scatter, r.lifted, weights.gate, start, columns, 0, geo.n)
        spread(scatter, r.lifted, weights.up, start, columns, columns, geo.n)
        scatter.send()
        scatters.append(scatter)
        start += columns
    squares.relay()
    for scatter in scatters:
        scatter.relay()
    if meanwhile is not None:
        meanwhile()
    scale = lax.rsqrt(squares.collect()[:, :1] / (width * geo.n) + EPS)
    for k, columns in enumerate(widths):
        sums = scatters[k].collect() * scale
        gate_sum, up_sum = sums[:, :columns], sums[:, columns:]
        gather = Gather(geo, at, r.passing[k], r.hidden[k])
        hidden = gate_sum / (1.0 + jnp.exp(-gate_sum)) * up_sum
        gather.rows[at.kv] = hidden.astype(gather.rows.dtype)
        gather.start()
        if gathers:
            gathers[-1].forward()
        gathers.append(gather)
    gathers[-1].forward()
    loads.down.wait()
    total, start = None, 0
    for gather, columns in zip(gathers, widths):
        gather.finish()
        term = jnp.dot(
            stacked(gather.rows), weights.down[start : start + columns, :], preferred_element_type=jnp.float32
        )
        total = term if total is None else total + term
        start += columns
    return total, [squares] + scatters + gathers


def start_loads(arrays, places, loading):
    copies = []
    for k, (src, dst) in enumerate(zip(arrays, places)):
        copies.append(pltpu.make_async_copy(src, dst, loading.at[k]))
        copies[-1].start()
    return type(places)(*copies)


def resting(arrays):
    return type(arrays)(*(pltpu.VMEM(a.shape, a.dtype) for a in arrays))


def whole(ref):
    cores, half, width = ref.shape
    return ref[...].astype(jnp.float32).reshape(cores * half, width)


class FirstArrays(NamedTuple):
    own: Any
    before_gain: Any
    gate: Any
    up: Any
    down: Any
    mix_gain: Any
    in_step: Any
    in_value: Any
    in_write: Any
    in_read: Any
    in_gate: Any
    step_bias: Any
    decay_log: Any
    skip_gain: Any
    group_gain: Any
    value_taps: Any
    write_taps: Any
    read_taps: Any
    value_window: Any
    write_window: Any
    read_window: Any
    scan: Any


class FirstRefs(NamedTuple):
    held: Any
    loading: Any
    pieces: Any
    piece_send: Any
    piece_recv: Any
    base: Any
    channel: Any
    reduce: Any
    aux: Any
    values: Any
    mixed: Any
    gates: Any
    pushes: Any
    decays: Any
    pushed: Any
    both: Any
    passing: Any


def first_kernel(geo, tree, mixes, *refs):
    count = len(FirstArrays._fields)
    sources, refs = refs[:count], refs[count:]
    first_out, state, value_next, write_next, read_next = refs[:5]
    mixed_rows, refs = refs[5 : 5 + len(mixes)], refs[5 + len(mixes) :]
    r = jax.tree.unflatten(tree, refs)
    at = place(geo)
    held = FirstArrays(*r.held, state)
    loads = start_loads(sources, held, r.loading)
    hail(geo, at)
    meet(geo)
    pieces = r.pieces
    own = held.own
    loads.own.wait()
    moves = []
    for d in range(1, geo.t):
        copy = remote(
            own, pieces.at[at.tp], r.piece_send.at[d - 1], r.piece_recv.at[d - 1],
            TP, lax.rem(at.tp + d, geo.t),
        )
        copy.start()
        moves.append(copy)
    pieces[at.tp] = own[...]
    loads.before_gain.wait()
    for copy in moves:
        copy.wait_recv()
    full = jnp.concatenate([pieces[k].astype(jnp.float32) for k in range(geo.t)], axis=1)
    base = r.base
    half = base.shape[1]
    for h in range(geo.cores):
        base[h] = full[h * half : (h + 1) * half].astype(base.dtype)
    total, pending = channel(
        geo, at, r.channel, full, held.before_gain, loads, held, functools.partial(halve, r, loads, state)
    )
    r.reduce.terms[...] = total
    moves += reduce_rows(geo, at, r.reduce, base, 0.5, first_out)
    features = full.shape[1] * geo.n
    aux = Scatter(geo, at, r.aux)
    loads.mix_gain.wait()
    lift(geo, r.channel, whole(first_out), held.mix_gain, aux)
    lifted = r.channel.lifted
    block = lifted.shape[0] // geo.n
    loads.in_step.wait()
    step = lax.dot_general(
        lifted[...], held.in_step[...], (((1,), (1,)), ((), ())),
        preferred_element_type=jnp.float32,
    )
    for i in range(geo.n):
        aux.put(i, slice(LANES, LANES + step.shape[1]), step[i * block : (i + 1) * block])
    aux.send()
    values = Scatter(geo, at, r.values)
    loads.in_value.wait()
    spread(values, lifted, held.in_value, 0, held.in_value.shape[1], 0, geo.n)
    values.send()
    mixed = Scatter(geo, at, r.mixed)
    offset = 0
    for load, weight in zip(loads[8:10], held[8:10]):
        load.wait()
        spread(mixed, lifted, weight, 0, weight.shape[1], offset, geo.n)
        offset += weight.shape[1]
    mixed.send()
    gates = Scatter(geo, at, r.gates)
    loads.in_gate.wait()
    spread(gates, lifted, held.in_gate, 0, held.in_gate.shape[1], 0, geo.n)
    gates.send()
    for scatter in (aux, values, mixed, gates):
        scatter.relay()
    for load in loads[11:-1]:
        load.wait()
    aux_sum = aux.collect()
    scale = lax.rsqrt(aux_sum[:, :1] / features + EPS)
    tables = prepare(r, held, aux_sum, scale, values.collect(), mixed.collect(), value_next, write_next, read_next)
    seen = [readout(r, tables, k) for k in range(sum(mixes))]
    gate_rows = (gates.collect() * scale).astype(jnp.bfloat16).astype(jnp.float32)
    group, gathers = 0, []
    for k, rows in enumerate(mixed_rows):
        gather = Gather(geo, at, r.passing[k], rows)
        span = rows.shape[2] // mixes[k]
        for j in range(mixes[k]):
            columns = slice(group * span, (group + 1) * span)
            part = (seen[group] + tables.direct[:, columns]) * silu(gate_rows[:, columns])
            mean = jnp.mean(part * part, axis=1, keepdims=True)
            part = part * lax.rsqrt(mean + EPS) * tables.gain[:, columns]
            rows[at.kv, :, j * span : (j + 1) * span] = part.astype(rows.dtype)
            group += 1
        gather.start()
        gathers.append(gather)
    for k in range(group - 1):
        advance(r, tables, state, k)
    for gather in gathers:
        gather.forward()
    advance(r, tables, state, group - 1)
    for gather in gathers:
        gather.finish()
    for copy in moves:
        copy.wait_send()
    for part in pending + [aux, values, mixed, gates] + gathers:
        part.drain()


class LastArrays(NamedTuple):
    gate: Any
    up: Any
    down: Any


class LastRefs(NamedTuple):
    held: Any
    loading: Any
    middle: Any
    channel: Any
    reduce: Any
    shares: Any
    kept: Any
    given: Any
    taken: Any
    end_send: Any
    end_recv: Any


def last_kernel(geo, tree, mixes, *refs):
    mixed_rows, refs = refs[: len(mixes)], refs[len(mixes) :]
    first_out, after_gain, out_weight = refs[:3]
    count = len(LastArrays._fields)
    sources, refs = refs[3 : 3 + count], refs[3 + count :]
    block_out = refs[0]
    r = jax.tree.unflatten(tree, refs[1:])
    at = place(geo)
    loads = start_loads(sources, r.held, r.loading)
    hail(geo, at)
    total, start = None, 0
    for rows in mixed_rows:
        stop = start + rows.shape[2]
        term = jnp.dot(
            stacked(rows), out_weight[start:stop, :], preferred_element_type=jnp.float32
        )
        total = term if total is None else total + term
        start = stop
    r.reduce.terms[...] = total
    meet(geo)
    middle = r.middle
    moves = reduce_rows(geo, at, r.reduce, first_out, 1.0, middle)
    full = whole(middle)
    width = block_out.shape[1]
    for k in range(geo.t):
        r.shares[k] = full[:, k * width : (k + 1) * width].astype(middle.dtype)
    total, pending = channel(geo, at, r.channel, full, after_gain, loads, r.held)
    for k in range(geo.t):
        part = total[:, k * width : (k + 1) * width]
        r.kept[k] = part
        r.given[k] = part.astype(jnp.bfloat16)
    ends = []
    for d in range(1, geo.t):
        peer = lax.rem(at.tp + d, geo.t)
        copy = remote(
            r.given.at[peer], r.taken.at[d - 1], r.end_send.at[d - 1], r.end_recv.at[d - 1],
            TP, peer,
        )
        copy.start()
        ends.append(copy)
    result = r.kept[at.tp]
    for d in range(1, geo.t):
        ends[d - 1].wait_recv()
        result = result + r.taken[d - 1].astype(jnp.float32)
    rest = r.shares[at.tp].astype(jnp.float32)
    block_out[...] = (rest + 0.5 * result).astype(block_out.dtype)
    for copy in moves + ends:
        copy.wait_send()
    for part in pending:
        part.drain()


def silu(v):
    return v / (1.0 + jnp.exp(-v))


def conv(window, fresh, taps, following):
    count = window.shape[0]
    wide = fresh.astype(jnp.float32)
    total = wide * taps[count : count + 1, :].astype(jnp.float32)
    for k in range(count):
        row = window[k]
        total = total + row.astype(jnp.float32) * taps[k : k + 1, :].astype(jnp.float32)
        if k:
            following[k - 1] = row
    following[count - 1] = fresh
    return silu(total)


def split(v):
    high = v.astype(jnp.bfloat16)
    return high, (v - high.astype(jnp.float32)).astype(jnp.bfloat16)


class Tables(NamedTuple):
    pushes: Any
    decays: Any
    write: Any
    read: Any
    direct: Any
    gain: Any
    decay: Any
    pushed: Any


def prepare(r, held, aux_sum, scale, value_sum, mixed_sum, value_next, write_next, read_next):
    block, heads = mixed_sum.shape[0], held.step_bias.shape[1]
    vectors = write_next.shape[2]
    fresh = (value_sum * scale).astype(jnp.bfloat16)
    value = conv(held.value_window, fresh, held.value_taps, value_next)
    fresh = (mixed_sum * scale).astype(jnp.bfloat16)
    write = conv(held.write_window, fresh[:, :vectors], held.write_taps, write_next)
    read = conv(held.read_window, fresh[:, vectors:], held.read_taps, read_next)
    raw = aux_sum[:, LANES : LANES + heads] * scale + held.step_bias[...]
    size = jnp.maximum(raw, 0.0) + jnp.log1p(jnp.exp(-jnp.abs(raw)))
    decay = jnp.exp(-size * jnp.exp(held.decay_log[...]))
    lane = lax.broadcasted_iota(jnp.int32, (1, 2 * HEAD_DIM), 1)

    def per_channel(v):
        return jnp.concatenate(
            [
                jnp.where(lane < HEAD_DIM, v[:, k : k + 1], v[:, k + 1 : k + 2])
                for k in range(0, heads, 2)
            ],
            axis=1,
        )

    pushed = value * per_channel(size)
    high, low = split(pushed)
    wide = high.astype(jnp.float32)
    pushes = jnp.concatenate([wide, wide, low.astype(jnp.float32)], axis=0)
    r.pushes[...] = pushes.T.astype(jnp.bfloat16)
    for h in range(heads):
        r.decays[h] = jnp.broadcast_to(decay[:, h : h + 1], (block, STATE))
    return Tables(
        r.pushes, r.decays, write, read,
        value * per_channel(held.skip_gain[...]), across(held.group_gain),
        per_channel(decay), pushed,
    )


def halve(r, loads, state):
    loads.scan.wait()
    block, heads = state.shape[0], state.shape[1]

    def step(h, carry):
        spot = pl.ds(pl.multiple_of(h * HEAD_DIM, HEAD_DIM), HEAD_DIM)
        for b in range(block):
            high, low = split(state[b, h])
            r.both[spot, 2 * b * STATE : (2 * b + 1) * STATE] = high
            r.both[spot, (2 * b + 1) * STATE : (2 * b + 2) * STATE] = low
        return carry

    lax.fori_loop(0, heads, step, 0)


def readout(r, tables, group):
    block = tables.write.shape[0]
    span = tables.direct.shape[1] // (tables.write.shape[1] // STATE)
    near = slice(group * STATE, (group + 1) * STATE)
    columns = slice(group * span, (group + 1) * span)
    reads = jnp.concatenate(
        [v.astype(jnp.float32) for v in split(tables.read[:, near])], axis=0
    ).T
    lane = lax.broadcasted_iota(jnp.int32, reads.shape, 1)
    picks = []
    for b in range(block):
        pick = jnp.where(lax.rem(lane, block) == b, reads, 0.0).astype(jnp.bfloat16)
        picks += [pick, pick]
    seen = jnp.dot(
        r.both[columns, :], jnp.concatenate(picks, axis=0), preferred_element_type=jnp.float32
    ).T
    met = jnp.sum(tables.write[:, near] * tables.read[:, near], axis=1, keepdims=True)
    old = (seen[:block] + seen[block:]) * tables.decay[:, columns]
    return old + tables.pushed[:, columns] * met


def advance(r, tables, state, group):
    block, heads = state.shape[0], state.shape[1]
    per_group = heads // (tables.write.shape[1] // STATE)
    span = per_group * HEAD_DIM
    near = slice(group * STATE, (group + 1) * STATE)
    row = lax.broadcasted_iota(jnp.int32, (3 * block, STATE), 0)
    high, low = split(tables.write[:, near])
    wide = high.astype(jnp.float32)
    stack = jnp.concatenate([wide, low.astype(jnp.float32), wide], axis=0)
    writes = jnp.concatenate(
        [jnp.where(lax.rem(row, block) == b, stack, 0.0) for b in range(block)], axis=1
    ).astype(jnp.bfloat16)
    pushed = r.pushed
    pushed[...] = jnp.dot(
        tables.pushes[group * span : (group + 1) * span, :], writes,
        preferred_element_type=jnp.float32,
    )
    for b in range(block):
        for j in range(per_group):
            h = group * per_group + j
            spot = slice(j * HEAD_DIM, (j + 1) * HEAD_DIM)
            fresh = tables.decays[h, b : b + 1, :] * state[b, h]
            state[b, h] = fresh + pushed[spot, b * STATE : (b + 1) * STATE]


VMEM = pl.BlockSpec(memory_space=pltpu.VMEM)
HBM = pl.BlockSpec(memory_space=pltpu.HBM)


def communicate(kernel, near, far, outs, scratch, ident, limit, micros):
    return pl.pallas_call(
        kernel,
        out_shape=outs,
        in_specs=[VMEM] * len(near) + [HBM] * len(far),
        out_specs=jax.tree.map(lambda _: VMEM, outs),
        scratch_shapes=scratch,
        compiler_params=pltpu.CompilerParams(
            collective_id=ident, has_side_effects=True, vmem_limit_bytes=limit
        ),
        cost_estimate=pl.CostEstimate(
            flops=0, bytes_accessed=micros * 3_000_000, transcendentals=0
        ),
    )(*near, *far)


def mix_groups(groups):
    chunks = min(MIX_CHUNKS, groups)
    return [groups // chunks + (k < groups % chunks) for k in range(chunks)]


def first_call(geo, by):
    shape = jax.ShapeDtypeStruct
    rows, width = by.own.shape[0], by.gate.shape[0]
    block = rows // geo.n
    inner, vectors = by.in_value.shape[1], by.in_write.shape[1]
    groups, heads = vectors // STATE, by.scan.shape[1]
    mixes = mix_groups(groups)
    span = inner // groups
    scratch = FirstRefs(
        tuple(resting(by))[:-1],
        sems(len(by)),
        pltpu.VMEM((geo.t,) + by.own.shape, by.own.dtype),
        sems(geo.t - 1), sems(geo.t - 1),
        pltpu.VMEM((geo.cores, rows // geo.cores, width), by.own.dtype),
        channel_refs(geo, rows, width, by.gate.shape[1]),
        reduce_refs(geo, rows, width),
        sum_refs(geo, block, LANES + by.in_step.shape[0], jnp.float32),
        sum_refs(geo, block, inner, jnp.bfloat16),
        sum_refs(geo, block, 2 * vectors, jnp.bfloat16),
        sum_refs(geo, block, inner, jnp.bfloat16),
        pltpu.VMEM((inner, 3 * block), jnp.bfloat16),
        pltpu.VMEM((heads, block, STATE), jnp.float32),
        pltpu.VMEM((span, block * STATE), jnp.float32),
        pltpu.VMEM((inner, 2 * block * STATE), jnp.bfloat16),
        [row_refs(geo) for _ in mixes],
    )
    leaves, tree = jax.tree.flatten(scratch)
    windows = (by.value_window, by.write_window, by.read_window)
    outs = (
        shape((geo.cores, rows // geo.cores, width), jnp.bfloat16),
        shape(by.scan.shape, by.scan.dtype),
        *(shape(w.shape, w.dtype) for w in windows),
        *(shape((geo.n, block, k * span), jnp.bfloat16) for k in mixes),
    )
    kernel = functools.partial(first_kernel, geo, tree, mixes)
    return mixes, communicate(kernel, (), by, outs, leaves, 0, 44 * 2**20, 50)


def last_call(geo, mixes, mixed_rows, first_out, after_gain, mixer_out, weights, share):
    rows = first_out.shape[0] * first_out.shape[1]
    width, hidden = weights.gate.shape
    scratch = LastRefs(
        resting(weights),
        sems(len(weights)),
        pltpu.VMEM(first_out.shape, first_out.dtype),
        channel_refs(geo, rows, width, hidden),
        reduce_refs(geo, rows, width),
        pltpu.VMEM((geo.t, rows, share), jnp.bfloat16),
        pltpu.VMEM((geo.t, rows, share), jnp.float32),
        pltpu.VMEM((geo.t, rows, share), jnp.bfloat16),
        pltpu.VMEM((max(1, geo.t - 1), rows, share), jnp.bfloat16),
        sems(geo.t - 1), sems(geo.t - 1),
    )
    leaves, tree = jax.tree.flatten(scratch)
    return communicate(
        functools.partial(last_kernel, geo, tree, mixes),
        (*mixed_rows, first_out, after_gain, mixer_out), weights,
        jax.ShapeDtypeStruct((rows, share), jnp.bfloat16), leaves, 1, 24 * 2**20, 36,
    )


def deliver_kernel(*refs):
    count = len(refs) // 2
    sems = refs[-1]
    copies = []
    for k in range(count):
        copy = pltpu.make_async_copy(refs[k], refs[count + k], sems.at[k])
        copy.start()
        copies.append(copy)
    for copy in copies:
        copy.wait()


def deliver(*arrays):
    return pl.pallas_call(
        deliver_kernel,
        out_shape=tuple(jax.ShapeDtypeStruct(a.shape, a.dtype) for a in arrays),
        in_specs=[VMEM] * len(arrays),
        out_specs=[HBM] * len(arrays),
        scratch_shapes=[pltpu.SemaphoreType.DMA((len(arrays),))],
        compiler_params=pltpu.CompilerParams(vmem_limit_bytes=12 * 2**20),
    )(*arrays)


def stay(arrays):
    return type(arrays)(*(pltpu.with_memory_space_constraint(a, pltpu.HBM) for a in arrays))


def local(
    geo,
    block_in,
    before_gain,
    before_gate,
    before_up,
    before_down,
    mix_gain,
    input_gate,
    input_value,
    input_write,
    input_read,
    input_step,
    step_bias,
    decay_log,
    skip_gain,
    value_taps,
    write_taps,
    read_taps,
    value_window,
    write_window,
    read_window,
    scan_state,
    group_gain,
    mixer_out,
    after_gain,
    after_gate,
    after_up,
    after_down,
):
    def line(vector):
        return vector.reshape(1, -1)

    def lanes(vector):
        return vector.reshape(-1, LANES)

    windows = [w.transpose(1, 0, 2) for w in (value_window, write_window, read_window)]
    mixes, (first_out, state_next, value_next, write_next, read_next, *mixed_rows) = first_call(
        geo,
        stay(FirstArrays(
            block_in, lanes(before_gain), before_gate, before_up, before_down, lanes(mix_gain),
            input_step.T, input_value, input_write, input_read, input_gate,
            line(step_bias), line(decay_log), line(skip_gain), lanes(group_gain),
            value_taps, write_taps, read_taps, *windows, scan_state,
        )),
    )
    block_out = last_call(
        geo, mixes, mixed_rows, first_out, lanes(after_gain), mixer_out,
        stay(LastArrays(after_gate, after_up, after_down)), block_in.shape[1],
    )
    block_out, state_next, *following = deliver(
        block_out, state_next, value_next, write_next, read_next
    )
    return (block_out, state_next, *(w.transpose(1, 0, 2) for w in following))


def solution(mesh):
    placed = (
        P(None, (KV, TP)),
        P(KV),
        P(KV, TP),
        P(KV, TP),
        P(TP, KV),
        P(KV),
        P(KV, TP),
        P(KV, TP),
        P(KV, TP),
        P(KV, TP),
        P(KV, TP),
        P(TP),
        P(TP),
        P(TP),
        P(None, TP),
        P(None, TP),
        P(None, TP),
        P(KV, None, TP),
        P(KV, None, TP),
        P(KV, None, TP),
        P(KV, TP, None, None),
        P(TP),
        P(TP, KV),
        P(KV),
        P(KV, TP),
        P(KV, TP),
        P(TP, KV),
    )
    return jax.shard_map(
        functools.partial(local, geometry(mesh)),
        mesh=mesh,
        in_specs=placed,
        out_specs=(
            P(None, (KV, TP)),
            P(KV, TP, None, None),
            P(KV, None, TP),
            P(KV, None, TP),
            P(KV, None, TP),
        ),
        check_vma=False,
    )
```

```python
import functools
from typing import Any, NamedTuple

import jax
import jax.numpy as jnp
from jax import lax
from jax.experimental import pallas as pl
from jax.experimental.pallas import tpu as pltpu
from jax.sharding import PartitionSpec as P

HEAD_DIM = 64
STATE = 128
EPS = 1e-06
TILE = 256
CHUNKS = 4
MIX_CHUNKS = 2
LANES = 128

MESH = pl.DeviceIdType.MESH
KV, TP = "kv", "tp"


class Geo(NamedTuple):
    n: int
    ny: int
    nz: int
    t: int
    nx: int
    cores: int


class At(NamedTuple):
    kv: Any
    z: Any
    y: Any
    tp: Any
    x: Any
    c: Any


def leading(line, key):
    keys = [key(d) for d in line]
    count = 1
    while count < len(keys) and keys[count] == keys[0]:
        count += 1
    return count if len(keys) % count == 0 else 1


def geometry(mesh):
    devices = mesh.devices
    n, t = mesh.shape[KV], mesh.shape[TP]
    if mesh.axis_names.index(KV) == 1:
        devices = devices.T
    ny = leading(devices[:, 0], lambda d: d.coords[2])
    cores = leading(devices[0], lambda d: tuple(d.coords))
    return Geo(n, ny, n // ny, t, t // cores, cores)


def place(geo):
    kv, tp = lax.axis_index(KV), lax.axis_index(TP)
    return At(kv, kv // geo.ny, lax.rem(kv, geo.ny), tp, tp // geo.cores, lax.rem(tp, geo.cores))


def sems(*shape):
    return pltpu.SemaphoreType.DMA(tuple(max(1, s) for s in shape))


def remote(src, dst, send_sem, recv_sem, axis, peer):
    return pltpu.make_async_remote_copy(
        src_ref=src,
        dst_ref=dst,
        send_sem=send_sem,
        recv_sem=recv_sem,
        device_id={axis: peer},
        device_id_type=MESH,
    )


def along_z(geo, z, k):
    if geo.nz & (geo.nz - 1):
        return lax.rem(z + k, geo.nz)
    bit = 1
    while bit < geo.nz:
        if k & bit:
            z = z + bit - 2 * bit * lax.rem(z // bit, 2)
        bit *= 2
    return z


def came_from(geo, z, k):
    return lax.rem(z + geo.nz - k, geo.nz) if geo.nz & (geo.nz - 1) else along_z(geo, z, k)


def hail(geo, at):
    barrier = pltpu.get_barrier_semaphore()
    for d in range(1, geo.t):
        peer = lax.rem(at.tp + d, geo.t)
        pl.semaphore_signal(barrier, inc=1, device_id={TP: peer}, device_id_type=MESH)
    for d in range(1, geo.ny):
        peer = at.z * geo.ny + lax.rem(at.y + d, geo.ny)
        pl.semaphore_signal(barrier, inc=1, device_id={KV: peer}, device_id_type=MESH)
    for e in range(1, geo.nz):
        peer = along_z(geo, at.z, e) * geo.ny + at.y
        pl.semaphore_signal(barrier, inc=1, device_id={KV: peer}, device_id_type=MESH)


def meet(geo):
    count = geo.t - 1 + geo.ny - 1 + geo.nz - 1
    pl.semaphore_wait(pltpu.get_barrier_semaphore(), count)


class SumRefs(NamedTuple):
    parts: Any
    staged: Any
    partial: Any
    landed: Any
    y_send: Any
    y_recv: Any
    z_send: Any
    z_recv: Any


def sum_refs(geo, block, width, dtype):
    across_y = (max(1, geo.ny - 1), geo.nz)
    along = (max(1, geo.nz - 1), block, width)
    return SumRefs(
        pltpu.VMEM((geo.ny, geo.nz, block, width), dtype),
        pltpu.VMEM(across_y + (block, width), dtype),
        pltpu.VMEM(along, dtype),
        pltpu.VMEM(along, dtype),
        sems(*across_y), sems(*across_y), sems(geo.nz - 1), sems(geo.nz - 1),
    )


class Scatter:
    def __init__(self, geo, at, refs):
        self.geo, self.at, self.refs = geo, at, refs
        self.parts, self.staged = refs.parts, refs.staged
        self.partial, self.landed = refs.partial, refs.landed
        self.first, self.second = {}, {}

    def put(self, i, columns, value):
        ny = self.geo.ny
        self.parts[i % ny, i // ny, :, columns] = value.astype(self.parts.dtype)

    def send(self):
        geo, at = self.geo, self.at
        for e in range(geo.nz - 1, -1, -1):
            zz = along_z(geo, at.z, e)
            for d in range(1, geo.ny):
                yy = lax.rem(at.y + d, geo.ny)
                copy = remote(
                    self.parts.at[yy, zz], self.staged.at[d - 1, e],
                    self.refs.y_send.at[d - 1, e], self.refs.y_recv.at[d - 1, e],
                    KV, at.z * geo.ny + yy,
                )
                copy.start()
                self.first[d, e] = copy

    def joined(self, e):
        geo, at = self.geo, self.at
        zz = along_z(geo, at.z, e)
        total = self.parts[at.y, zz].astype(jnp.float32)
        for d in range(1, geo.ny):
            self.first[d, e].wait_recv()
            total = total + self.staged[d - 1, e].astype(jnp.float32)
        return total, zz

    def relay(self):
        geo, at = self.geo, self.at
        for e in range(geo.nz - 1, 0, -1):
            total, zz = self.joined(e)
            self.partial[e - 1] = total.astype(self.partial.dtype)
            copy = remote(
                self.partial.at[e - 1], self.landed.at[e - 1],
                self.refs.z_send.at[e - 1], self.refs.z_recv.at[e - 1],
                KV, zz * geo.ny + at.y,
            )
            copy.start()
            self.second[e] = copy

    def collect(self):
        total, _ = self.joined(0)
        for e in range(self.geo.nz - 1, 0, -1):
            self.second[e].wait_recv()
            total = total + self.landed[e - 1].astype(jnp.float32)
        return total

    def drain(self):
        for copy in list(self.first.values()) + list(self.second.values()):
            copy.wait_send()


class RowRefs(NamedTuple):
    z_send: Any
    z_recv: Any
    y_send: Any
    y_recv: Any


def row_refs(geo):
    return RowRefs(
        sems(geo.nz - 1), sems(geo.nz - 1), sems(geo.ny - 1, geo.nz), sems(geo.ny - 1, geo.nz)
    )


class Gather:
    def __init__(self, geo, at, refs, rows):
        self.geo, self.at, self.refs, self.rows = geo, at, refs, rows
        self.first, self.second = {}, {}

    def pass_on(self, src, index, e):
        geo, at = self.geo, self.at
        for d in range(1, geo.ny):
            yy = lax.rem(at.y + d, geo.ny)
            copy = remote(
                src, self.rows.at[index],
                self.refs.y_send.at[d - 1, e], self.refs.y_recv.at[d - 1, e],
                KV, at.z * geo.ny + yy,
            )
            copy.start()
            self.second[d, e] = copy

    def start(self):
        geo, at = self.geo, self.at
        src = self.rows.at[at.kv]
        for e in range(geo.nz - 1, 0, -1):
            zz = along_z(geo, at.z, e)
            copy = remote(
                src, self.rows.at[at.kv], self.refs.z_send.at[e - 1], self.refs.z_recv.at[e - 1],
                KV, zz * geo.ny + at.y,
            )
            copy.start()
            self.first[e] = copy
        self.pass_on(src, at.kv, 0)

    def forward(self):
        geo, at = self.geo, self.at
        for e in range(1, geo.nz):
            self.first[e].wait_recv()
            index = came_from(geo, at.z, e) * geo.ny + at.y
            self.pass_on(self.rows.at[index], index, e)

    def finish(self):
        for copy in self.second.values():
            copy.wait_recv()

    def drain(self):
        for copy in list(self.first.values()) + list(self.second.values()):
            copy.wait_send()


def stacked(rows):
    n, block, width = rows.shape
    wide = rows[...].astype(jnp.float32).reshape(n * block, width)
    return wide.astype(rows.dtype)


class ReduceRefs(NamedTuple):
    terms: Any
    pair: Any
    mine: Any
    far: Any
    near_send: Any
    near_recv: Any
    far_send: Any
    far_recv: Any


def reduce_refs(geo, rows, width):
    half = rows // geo.cores
    across_x = (max(1, geo.nx - 1), geo.cores)
    return ReduceRefs(
        pltpu.VMEM((rows, width), jnp.float32),
        pltpu.VMEM((max(1, geo.cores - 1), rows, width), jnp.float32),
        pltpu.VMEM((geo.cores, half, width), jnp.bfloat16),
        pltpu.VMEM(across_x + (half, width), jnp.bfloat16),
        sems(geo.cores - 1), sems(geo.cores - 1), sems(*across_x), sems(*across_x),
    )


def reduce_rows(geo, at, r, base, weight, out):
    terms, pair, mine, far = r.terms, r.pair, r.mine, r.far
    sends = []
    for q in range(1, geo.cores):
        copy = remote(
            terms, pair.at[q - 1], r.near_send.at[q - 1], r.near_recv.at[q - 1],
            TP, at.x * geo.cores + lax.rem(at.c + q, geo.cores),
        )
        copy.start()
        sends.append(copy)
    half = mine.shape[1]
    for copy in sends:
        copy.wait_recv()
    for h in range(geo.cores):
        total = terms[h * half : (h + 1) * half]
        for q in range(1, geo.cores):
            total = total + pair[q - 1, h * half : (h + 1) * half]
        mine[h] = total.astype(mine.dtype)
    crossing = {}
    for dx in range(1, geo.nx):
        for q in range(geo.cores):
            copy = remote(
                mine.at[at.c], far.at[dx - 1, q],
                r.far_send.at[dx - 1, q], r.far_recv.at[dx - 1, q],
                TP, lax.rem(at.x + dx, geo.nx) * geo.cores + lax.rem(at.c + q, geo.cores),
            )
            copy.start()
            crossing[dx, q] = copy
    for q in range(geo.cores):
        h = lax.rem(at.c + geo.cores - q, geo.cores)
        total = mine[h].astype(jnp.float32)
        for dx in range(1, geo.nx):
            crossing[dx, q].wait_recv()
            total = total + far[dx - 1, q].astype(jnp.float32)
        out[h] = (base[h].astype(jnp.float32) + weight * total).astype(out.dtype)
    return sends + list(crossing.values())


def tiles_of(width):
    size = TILE if width % TILE == 0 else 128
    return size, width // size


def chunk_widths(width):
    size, count = tiles_of(width)
    chunks = min(CHUNKS, count)
    return [size * (count // chunks + (k < count % chunks)) for k in range(chunks)]


def spread(scatter, lifted, weight, start, width, offset, n):
    size, count = tiles_of(width)
    block = lifted.shape[0] // n
    for k in range(count):
        tile = jnp.dot(
            lifted[...], weight[:, start + k * size : start + (k + 1) * size],
            preferred_element_type=jnp.float32,
        )
        columns = slice(offset + k * size, offset + (k + 1) * size)
        for i in range(n):
            scatter.put(i, columns, tile[i * block : (i + 1) * block])


def across(gain):
    wide = gain[...].astype(jnp.float32)
    return jnp.concatenate([wide[k : k + 1] for k in range(wide.shape[0])], axis=1)


def lift(geo, r, full, gain, aux):
    r.lifted[...] = (full * across(gain)).astype(jnp.bfloat16)
    squares = jnp.sum(full * full, axis=1, keepdims=True)
    block = full.shape[0] // geo.n
    for i in range(geo.n):
        part = squares[i * block : (i + 1) * block]
        aux.put(i, slice(0, 128), jnp.broadcast_to(part, (block, 128)))


class ChannelRefs(NamedTuple):
    lifted: Any
    squares: Any
    sums: Any
    hidden: Any
    passing: Any


def channel_refs(geo, rows, width, hidden):
    block = rows // geo.n
    widths = chunk_widths(hidden)
    return ChannelRefs(
        pltpu.VMEM((rows, width), jnp.bfloat16),
        sum_refs(geo, block, LANES, jnp.float32),
        [sum_refs(geo, block, 2 * columns, jnp.bfloat16) for columns in widths],
        [pltpu.VMEM((geo.n, block, columns), jnp.bfloat16) for columns in widths],
        [row_refs(geo) for _ in widths],
    )


def channel(geo, at, r, full, gain, loads, weights, meanwhile=None):
    rows, width = full.shape
    widths = chunk_widths(weights.gate.shape[1])
    squares = Scatter(geo, at, r.squares)
    lift(geo, r, full, gain, squares)
    squares.send()
    loads.gate.wait()
    loads.up.wait()
    scatters, gathers = [], []
    start = 0
    for k, columns in enumerate(widths):
        scatter = Scatter(geo, at, r.sums[k])
        spread(scatter, r.lifted, weights.gate, start, columns, 0, geo.n)
        spread(scatter, r.lifted, weights.up, start, columns, columns, geo.n)
        scatter.send()
        scatters.append(scatter)
        start += columns
    squares.relay()
    for scatter in scatters:
        scatter.relay()
    if meanwhile is not None:
        meanwhile()
    scale = lax.rsqrt(squares.collect()[:, :1] / (width * geo.n) + EPS)
    for k, columns in enumerate(widths):
        sums = scatters[k].collect() * scale
        gate_sum, up_sum = sums[:, :columns], sums[:, columns:]
        gather = Gather(geo, at, r.passing[k], r.hidden[k])
        hidden = gate_sum / (1.0 + jnp.exp(-gate_sum)) * up_sum
        gather.rows[at.kv] = hidden.astype(gather.rows.dtype)
        gather.start()
        if gathers:
            gathers[-1].forward()
        gathers.append(gather)
    gathers[-1].forward()
    loads.down.wait()
    total, start = None, 0
    for gather, columns in zip(gathers, widths):
        gather.finish()
        term = jnp.dot(
            stacked(gather.rows), weights.down[start : start + columns, :], preferred_element_type=jnp.float32
        )
        total = term if total is None else total + term
        start += columns
    return total, [squares] + scatters + gathers


def start_loads(arrays, places, loading, first):
    copies = []
    for k, (src, dst) in enumerate(zip(arrays, places)):
        copies.append(pltpu.make_async_copy(src, dst, loading.at[k]))
        if k < first:
            copies[-1].start()
    return type(places)(*copies)


def resting(arrays):
    return type(arrays)(*(pltpu.VMEM(a.shape, a.dtype) for a in arrays))


def whole(ref):
    cores, half, width = ref.shape
    return ref[...].astype(jnp.float32).reshape(cores * half, width)


class FirstArrays(NamedTuple):
    own: Any
    before_gain: Any
    gate: Any
    up: Any
    down: Any
    mix_gain: Any
    in_step: Any
    in_value: Any
    in_write: Any
    in_read: Any
    in_gate: Any
    step_bias: Any
    decay_log: Any
    skip_gain: Any
    group_gain: Any
    value_taps: Any
    write_taps: Any
    read_taps: Any
    value_window: Any
    write_window: Any
    read_window: Any
    scan: Any


class FirstRefs(NamedTuple):
    held: Any
    loading: Any
    pieces: Any
    piece_send: Any
    piece_recv: Any
    base: Any
    channel: Any
    reduce: Any
    aux: Any
    values: Any
    mixed: Any
    gates: Any
    pushes: Any
    decays: Any
    pushed: Any
    both: Any
    passing: Any


def first_kernel(geo, tree, mixes, *refs):
    count = len(FirstArrays._fields)
    sources, refs = refs[:count], refs[count:]
    first_out, state, value_next, write_next, read_next = refs[:5]
    mixed_rows, refs = refs[5 : 5 + len(mixes)], refs[5 + len(mixes) :]
    r = jax.tree.unflatten(tree, refs)
    at = place(geo)
    held = FirstArrays(*r.held, state)
    loads = start_loads(sources, held, r.loading, 4)
    hail(geo, at)
    meet(geo)
    pieces = r.pieces
    own = held.own
    loads.own.wait()
    moves = []
    for d in range(1, geo.t):
        copy = remote(
            own, pieces.at[at.tp], r.piece_send.at[d - 1], r.piece_recv.at[d - 1],
            TP, lax.rem(at.tp + d, geo.t),
        )
        copy.start()
        moves.append(copy)
    pieces[at.tp] = own[...]
    loads.before_gain.wait()
    for copy in moves:
        copy.wait_recv()
    for load in loads[4:]:
        load.start()
    full = jnp.concatenate([pieces[k].astype(jnp.float32) for k in range(geo.t)], axis=1)
    base = r.base
    half = base.shape[1]
    for h in range(geo.cores):
        base[h] = full[h * half : (h + 1) * half].astype(base.dtype)
    total, pending = channel(
        geo, at, r.channel, full, held.before_gain, loads, held, functools.partial(halve, r, loads, state)
    )
    r.reduce.terms[...] = total
    moves += reduce_rows(geo, at, r.reduce, base, 0.5, first_out)
    features = full.shape[1] * geo.n
    aux = Scatter(geo, at, r.aux)
    loads.mix_gain.wait()
    lift(geo, r.channel, whole(first_out), held.mix_gain, aux)
    lifted = r.channel.lifted
    block = lifted.shape[0] // geo.n
    loads.in_step.wait()
    step = lax.dot_general(
        lifted[...], held.in_step[...], (((1,), (1,)), ((), ())),
        preferred_element_type=jnp.float32,
    )
    for i in range(geo.n):
        aux.put(i, slice(LANES, LANES + step.shape[1]), step[i * block : (i + 1) * block])
    aux.send()
    values = Scatter(geo, at, r.values)
    loads.in_value.wait()
    spread(values, lifted, held.in_value, 0, held.in_value.shape[1], 0, geo.n)
    values.send()
    mixed = Scatter(geo, at, r.mixed)
    offset = 0
    for load, weight in zip(loads[8:10], held[8:10]):
        load.wait()
        spread(mixed, lifted, weight, 0, weight.shape[1], offset, geo.n)
        offset += weight.shape[1]
    mixed.send()
    gates = Scatter(geo, at, r.gates)
    loads.in_gate.wait()
    spread(gates, lifted, held.in_gate, 0, held.in_gate.shape[1], 0, geo.n)
    gates.send()
    for scatter in (aux, values, mixed, gates):
        scatter.relay()
    for load in loads[11:-1]:
        load.wait()
    aux_sum = aux.collect()
    scale = lax.rsqrt(aux_sum[:, :1] / features + EPS)
    tables = prepare(r, held, aux_sum, scale, values.collect(), mixed.collect(), value_next, write_next, read_next)
    seen = [readout(r, tables, k) for k in range(sum(mixes))]
    gate_rows = (gates.collect() * scale).astype(jnp.bfloat16).astype(jnp.float32)
    group, gathers = 0, []
    for k, rows in enumerate(mixed_rows):
        gather = Gather(geo, at, r.passing[k], rows)
        span = rows.shape[2] // mixes[k]
        for j in range(mixes[k]):
            columns = slice(group * span, (group + 1) * span)
            part = (seen[group] + tables.direct[:, columns]) * silu(gate_rows[:, columns])
            mean = jnp.mean(part * part, axis=1, keepdims=True)
            part = part * lax.rsqrt(mean + EPS) * tables.gain[:, columns]
            rows[at.kv, :, j * span : (j + 1) * span] = part.astype(rows.dtype)
            group += 1
        gather.start()
        gathers.append(gather)
    for k in range(group - 1):
        advance(r, tables, state, k)
    for gather in gathers:
        gather.forward()
    advance(r, tables, state, group - 1)
    for gather in gathers:
        gather.finish()
    for copy in moves:
        copy.wait_send()
    for part in pending + [aux, values, mixed, gates] + gathers:
        part.drain()


class LastArrays(NamedTuple):
    gate: Any
    up: Any
    down: Any


class LastRefs(NamedTuple):
    held: Any
    loading: Any
    middle: Any
    channel: Any
    reduce: Any
    shares: Any
    kept: Any
    given: Any
    taken: Any
    end_send: Any
    end_recv: Any


def last_kernel(geo, tree, mixes, *refs):
    mixed_rows, refs = refs[: len(mixes)], refs[len(mixes) :]
    first_out, after_gain, out_weight = refs[:3]
    count = len(LastArrays._fields)
    sources, refs = refs[3 : 3 + count], refs[3 + count :]
    block_out = refs[0]
    r = jax.tree.unflatten(tree, refs[1:])
    at = place(geo)
    loads = start_loads(sources, r.held, r.loading, count)
    hail(geo, at)
    total, start = None, 0
    for rows in mixed_rows:
        stop = start + rows.shape[2]
        term = jnp.dot(
            stacked(rows), out_weight[start:stop, :], preferred_element_type=jnp.float32
        )
        total = term if total is None else total + term
        start = stop
    r.reduce.terms[...] = total
    meet(geo)
    middle = r.middle
    moves = reduce_rows(geo, at, r.reduce, first_out, 1.0, middle)
    full = whole(middle)
    width = block_out.shape[1]
    for k in range(geo.t):
        r.shares[k] = full[:, k * width : (k + 1) * width].astype(middle.dtype)
    total, pending = channel(geo, at, r.channel, full, after_gain, loads, r.held)
    for k in range(geo.t):
        part = total[:, k * width : (k + 1) * width]
        r.kept[k] = part
        r.given[k] = part.astype(jnp.bfloat16)
    ends = []
    for d in range(1, geo.t):
        peer = lax.rem(at.tp + d, geo.t)
        copy = remote(
            r.given.at[peer], r.taken.at[d - 1], r.end_send.at[d - 1], r.end_recv.at[d - 1],
            TP, peer,
        )
        copy.start()
        ends.append(copy)
    result = r.kept[at.tp]
    for d in range(1, geo.t):
        ends[d - 1].wait_recv()
        result = result + r.taken[d - 1].astype(jnp.float32)
    rest = r.shares[at.tp].astype(jnp.float32)
    block_out[...] = (rest + 0.5 * result).astype(block_out.dtype)
    for copy in moves + ends:
        copy.wait_send()
    for part in pending:
        part.drain()


def silu(v):
    return v / (1.0 + jnp.exp(-v))


def conv(window, fresh, taps, following):
    count = window.shape[0]
    wide = fresh.astype(jnp.float32)
    total = wide * taps[count : count + 1, :].astype(jnp.float32)
    for k in range(count):
        row = window[k]
        total = total + row.astype(jnp.float32) * taps[k : k + 1, :].astype(jnp.float32)
        if k:
            following[k - 1] = row
    following[count - 1] = fresh
    return silu(total)


def split(v):
    high = v.astype(jnp.bfloat16)
    return high, (v - high.astype(jnp.float32)).astype(jnp.bfloat16)


class Tables(NamedTuple):
    pushes: Any
    decays: Any
    write: Any
    read: Any
    direct: Any
    gain: Any
    decay: Any
    pushed: Any


def prepare(r, held, aux_sum, scale, value_sum, mixed_sum, value_next, write_next, read_next):
    block, heads = mixed_sum.shape[0], held.step_bias.shape[1]
    vectors = write_next.shape[2]
    fresh = (value_sum * scale).astype(jnp.bfloat16)
    value = conv(held.value_window, fresh, held.value_taps, value_next)
    fresh = (mixed_sum * scale).astype(jnp.bfloat16)
    write = conv(held.write_window, fresh[:, :vectors], held.write_taps, write_next)
    read = conv(held.read_window, fresh[:, vectors:], held.read_taps, read_next)
    raw = aux_sum[:, LANES : LANES + heads] * scale + held.step_bias[...]
    size = jnp.maximum(raw, 0.0) + jnp.log1p(jnp.exp(-jnp.abs(raw)))
    decay = jnp.exp(-size * jnp.exp(held.decay_log[...]))
    lane = lax.broadcasted_iota(jnp.int32, (1, 2 * HEAD_DIM), 1)

    def per_channel(v):
        return jnp.concatenate(
            [
                jnp.where(lane < HEAD_DIM, v[:, k : k + 1], v[:, k + 1 : k + 2])
                for k in range(0, heads, 2)
            ],
            axis=1,
        )

    pushed = value * per_channel(size)
    high, low = split(pushed)
    wide = high.astype(jnp.float32)
    pushes = jnp.concatenate([wide, wide, low.astype(jnp.float32)], axis=0)
    r.pushes[...] = pushes.T.astype(jnp.bfloat16)
    for h in range(heads):
        r.decays[h] = jnp.broadcast_to(decay[:, h : h + 1], (block, STATE))
    return Tables(
        r.pushes, r.decays, write, read,
        value * per_channel(held.skip_gain[...]), across(held.group_gain),
        per_channel(decay), pushed,
    )


def halve(r, loads, state):
    loads.scan.wait()
    block, heads = state.shape[0], state.shape[1]

    def step(h, carry):
        spot = pl.ds(pl.multiple_of(h * HEAD_DIM, HEAD_DIM), HEAD_DIM)
        for b in range(block):
            high, low = split(state[b, h])
            r.both[spot, 2 * b * STATE : (2 * b + 1) * STATE] = high
            r.both[spot, (2 * b + 1) * STATE : (2 * b + 2) * STATE] = low
        return carry

    lax.fori_loop(0, heads, step, 0)


def readout(r, tables, group):
    block = tables.write.shape[0]
    span = tables.direct.shape[1] // (tables.write.shape[1] // STATE)
    near = slice(group * STATE, (group + 1) * STATE)
    columns = slice(group * span, (group + 1) * span)
    reads = jnp.concatenate(
        [v.astype(jnp.float32) for v in split(tables.read[:, near])], axis=0
    ).T
    lane = lax.broadcasted_iota(jnp.int32, reads.shape, 1)
    picks = []
    for b in range(block):
        pick = jnp.where(lax.rem(lane, block) == b, reads, 0.0).astype(jnp.bfloat16)
        picks += [pick, pick]
    seen = jnp.dot(
        r.both[columns, :], jnp.concatenate(picks, axis=0), preferred_element_type=jnp.float32
    ).T
    met = jnp.sum(tables.write[:, near] * tables.read[:, near], axis=1, keepdims=True)
    old = (seen[:block] + seen[block:]) * tables.decay[:, columns]
    return old + tables.pushed[:, columns] * met


def advance(r, tables, state, group):
    block, heads = state.shape[0], state.shape[1]
    per_group = heads // (tables.write.shape[1] // STATE)
    span = per_group * HEAD_DIM
    near = slice(group * STATE, (group + 1) * STATE)
    row = lax.broadcasted_iota(jnp.int32, (3 * block, STATE), 0)
    high, low = split(tables.write[:, near])
    wide = high.astype(jnp.float32)
    stack = jnp.concatenate([wide, low.astype(jnp.float32), wide], axis=0)
    writes = jnp.concatenate(
        [jnp.where(lax.rem(row, block) == b, stack, 0.0) for b in range(block)], axis=1
    ).astype(jnp.bfloat16)
    pushed = r.pushed
    pushed[...] = jnp.dot(
        tables.pushes[group * span : (group + 1) * span, :], writes,
        preferred_element_type=jnp.float32,
    )
    for b in range(block):
        for j in range(per_group):
            h = group * per_group + j
            spot = slice(j * HEAD_DIM, (j + 1) * HEAD_DIM)
            fresh = tables.decays[h, b : b + 1, :] * state[b, h]
            state[b, h] = fresh + pushed[spot, b * STATE : (b + 1) * STATE]


VMEM = pl.BlockSpec(memory_space=pltpu.VMEM)
HBM = pl.BlockSpec(memory_space=pltpu.HBM)


def communicate(kernel, near, far, outs, scratch, ident, limit, micros):
    return pl.pallas_call(
        kernel,
        out_shape=outs,
        in_specs=[VMEM] * len(near) + [HBM] * len(far),
        out_specs=jax.tree.map(lambda _: VMEM, outs),
        scratch_shapes=scratch,
        compiler_params=pltpu.CompilerParams(
            collective_id=ident, has_side_effects=True, vmem_limit_bytes=limit
        ),
        cost_estimate=pl.CostEstimate(
            flops=0, bytes_accessed=micros * 3_000_000, transcendentals=0
        ),
    )(*near, *far)


def mix_groups(groups):
    chunks = min(MIX_CHUNKS, groups)
    return [groups // chunks + (k < groups % chunks) for k in range(chunks)]


def first_call(geo, by):
    shape = jax.ShapeDtypeStruct
    rows, width = by.own.shape[0], by.gate.shape[0]
    block = rows // geo.n
    inner, vectors = by.in_value.shape[1], by.in_write.shape[1]
    groups, heads = vectors // STATE, by.scan.shape[1]
    mixes = mix_groups(groups)
    span = inner // groups
    scratch = FirstRefs(
        tuple(resting(by))[:-1],
        sems(len(by)),
        pltpu.VMEM((geo.t,) + by.own.shape, by.own.dtype),
        sems(geo.t - 1), sems(geo.t - 1),
        pltpu.VMEM((geo.cores, rows // geo.cores, width), by.own.dtype),
        channel_refs(geo, rows, width, by.gate.shape[1]),
        reduce_refs(geo, rows, width),
        sum_refs(geo, block, LANES + by.in_step.shape[0], jnp.float32),
        sum_refs(geo, block, inner, jnp.bfloat16),
        sum_refs(geo, block, 2 * vectors, jnp.bfloat16),
        sum_refs(geo, block, inner, jnp.bfloat16),
        pltpu.VMEM((inner, 3 * block), jnp.bfloat16),
        pltpu.VMEM((heads, block, STATE), jnp.float32),
        pltpu.VMEM((span, block * STATE), jnp.float32),
        pltpu.VMEM((inner, 2 * block * STATE), jnp.bfloat16),
        [row_refs(geo) for _ in mixes],
    )
    leaves, tree = jax.tree.flatten(scratch)
    windows = (by.value_window, by.write_window, by.read_window)
    outs = (
        shape((geo.cores, rows // geo.cores, width), jnp.bfloat16),
        shape(by.scan.shape, by.scan.dtype),
        *(shape(w.shape, w.dtype) for w in windows),
        *(shape((geo.n, block, k * span), jnp.bfloat16) for k in mixes),
    )
    kernel = functools.partial(first_kernel, geo, tree, mixes)
    return mixes, communicate(kernel, (), by, outs, leaves, 0, 44 * 2**20, 50)


def last_call(geo, mixes, mixed_rows, first_out, after_gain, mixer_out, weights, share):
    rows = first_out.shape[0] * first_out.shape[1]
    width, hidden = weights.gate.shape
    scratch = LastRefs(
        resting(weights),
        sems(len(weights)),
        pltpu.VMEM(first_out.shape, first_out.dtype),
        channel_refs(geo, rows, width, hidden),
        reduce_refs(geo, rows, width),
        pltpu.VMEM((geo.t, rows, share), jnp.bfloat16),
        pltpu.VMEM((geo.t, rows, share), jnp.float32),
        pltpu.VMEM((geo.t, rows, share), jnp.bfloat16),
        pltpu.VMEM((max(1, geo.t - 1), rows, share), jnp.bfloat16),
        sems(geo.t - 1), sems(geo.t - 1),
    )
    leaves, tree = jax.tree.flatten(scratch)
    return communicate(
        functools.partial(last_kernel, geo, tree, mixes),
        (*mixed_rows, first_out, after_gain, mixer_out), weights,
        jax.ShapeDtypeStruct((rows, share), jnp.bfloat16), leaves, 1, 24 * 2**20, 36,
    )


def deliver_kernel(*refs):
    count = len(refs) // 2
    sems = refs[-1]
    copies = []
    for k in range(count):
        copy = pltpu.make_async_copy(refs[k], refs[count + k], sems.at[k])
        copy.start()
        copies.append(copy)
    for copy in copies:
        copy.wait()


def deliver(*arrays):
    return pl.pallas_call(
        deliver_kernel,
        out_shape=tuple(jax.ShapeDtypeStruct(a.shape, a.dtype) for a in arrays),
        in_specs=[VMEM] * len(arrays),
        out_specs=[HBM] * len(arrays),
        scratch_shapes=[pltpu.SemaphoreType.DMA((len(arrays),))],
        compiler_params=pltpu.CompilerParams(vmem_limit_bytes=12 * 2**20),
    )(*arrays)


def stay(arrays):
    return type(arrays)(*(pltpu.with_memory_space_constraint(a, pltpu.HBM) for a in arrays))


def local(
    geo,
    block_in,
    before_gain,
    before_gate,
    before_up,
    before_down,
    mix_gain,
    input_gate,
    input_value,
    input_write,
    input_read,
    input_step,
    step_bias,
    decay_log,
    skip_gain,
    value_taps,
    write_taps,
    read_taps,
    value_window,
    write_window,
    read_window,
    scan_state,
    group_gain,
    mixer_out,
    after_gain,
    after_gate,
    after_up,
    after_down,
):
    def line(vector):
        return vector.reshape(1, -1)

    def lanes(vector):
        return vector.reshape(-1, LANES)

    windows = [w.transpose(1, 0, 2) for w in (value_window, write_window, read_window)]
    mixes, (first_out, state_next, value_next, write_next, read_next, *mixed_rows) = first_call(
        geo,
        stay(FirstArrays(
            block_in, lanes(before_gain), before_gate, before_up, before_down, lanes(mix_gain),
            input_step.T, input_value, input_write, input_read, input_gate,
            line(step_bias), line(decay_log), line(skip_gain), lanes(group_gain),
            value_taps, write_taps, read_taps, *windows, scan_state,
        )),
    )
    block_out = last_call(
        geo, mixes, mixed_rows, first_out, lanes(after_gain), mixer_out,
        stay(LastArrays(after_gate, after_up, after_down)), block_in.shape[1],
    )
    block_out, state_next, *following = deliver(
        block_out, state_next, value_next, write_next, read_next
    )
    return (block_out, state_next, *(w.transpose(1, 0, 2) for w in following))


def solution(mesh):
    placed = (
        P(None, (KV, TP)),
        P(KV),
        P(KV, TP),
        P(KV, TP),
        P(TP, KV),
        P(KV),
        P(KV, TP),
        P(KV, TP),
        P(KV, TP),
        P(KV, TP),
        P(KV, TP),
        P(TP),
        P(TP),
        P(TP),
        P(None, TP),
        P(None, TP),
        P(None, TP),
        P(KV, None, TP),
        P(KV, None, TP),
        P(KV, None, TP),
        P(KV, TP, None, None),
        P(TP),
        P(TP, KV),
        P(KV),
        P(KV, TP),
        P(KV, TP),
        P(TP, KV),
    )
    return jax.shard_map(
        functools.partial(local, geometry(mesh)),
        mesh=mesh,
        in_specs=placed,
        out_specs=(
            P(None, (KV, TP)),
            P(KV, TP, None, None),
            P(KV, None, TP),
            P(KV, None, TP),
            P(KV, None, TP),
        ),
        check_vma=False,
    )
```
